128 devices in a mesh: fs: 32 (over z, y, core), tp: 4 (over x).
Axes of the slice: x: 4, y: 4, z: 4, core: 2. Of those that a mesh axis runs over, the one named last changes fastest.
Arguments:
- first_map: bfloat16 [24576, 2048], P('fs', 'tp'), may hold values from -6 to 6
- second_map: bfloat16 [24576, 2048], P('fs', 'tp'), may hold values from -6 to 6
- lambda_head: float32 [16], P('tp'), may hold values from 0.3 to 0.8
- head_gain: float32 [2048], P('tp'), may hold values from 0.1 to 1.9
- cot_output: bfloat16 [24576, 4096], P('fs'), may hold values from -6 to 6
- layer_input: bfloat16 [24576, 4096], P('fs'), may hold values from -6 to 6
- cot_values: bfloat16 [24576, 2048], P('fs', 'tp'), may hold values from -16 to 16
- factor_value: bfloat16 [4096, 256], P('fs'), may hold values from -1 to 1
- factor_output: bfloat16 [4096, 256], P('fs'), may hold values from -1 to 1
- weight_value: float32 [4096, 2048], P('fs', 'tp'), may hold values from -6 to 6
- weight_output: float32 [2048, 4096], P('tp', 'fs'), may hold values from -6 to 6
- first_value: float32 [256, 2048], P('fs', 'tp'), may hold values from -6 to 6
- second_value: float32 [256, 2048], P('fs', 'tp'), may hold values from 0.05 to 1
- first_output: float32 [256, 2048], P('fs', 'tp'), may hold values from -6 to 6
- second_output: float32 [256, 2048], P('fs', 'tp'), may hold values from 0.05 to 1
Outputs:
- new_weight_value: float32 [4096, 2048], P('fs', 'tp')
- new_first_value: float32 [256, 2048], P('fs', 'tp')
- new_second_value: float32 [256, 2048], P('fs', 'tp')
- copy_value: bfloat16 [4096, 2048], P(None, 'tp')
- new_weight_output: float32 [2048, 4096], P('tp', 'fs')
- new_first_output: float32 [256, 2048], P('fs', 'tp')
- new_second_output: float32 [256, 2048], P('fs', 'tp')
- copy_output: bfloat16 [2048, 4096], P('tp')
The draws below stay inside these ranges and needn't reach their ends.
All inputs are finite; a program needn't handle non-finite values.
Results may differ from the reference program's by a relative error of at most 0.002.
Values may be sent and summed in bfloat16 or wider, within the bound.
A program may use at most 128 MiB of HBM per device.

```python
import math
import jax
import jax.numpy as jnp
from jax import lax

D = 4096
HEADS = 16
RANK = 256
HV = 2048
TOKENS = 24576


def rising_draw(key, count_rows, count_cols, top_scale):
    base = jnp.clip(jax.random.normal(key, (count_rows, count_cols), jnp.float32), -4.0, 4.0)
    column = jnp.arange(count_cols, dtype=jnp.float32) / max(count_cols - 1, 1)
    return base * (top_scale ** column)[None, :]


def draw_cot_values(key, part):
    return rising_draw(jax.random.fold_in(key, 11), TOKENS, HV, 4.0).astype(jnp.bfloat16)


def draw_factor_value(key, part):
    return (rising_draw(jax.random.fold_in(key, 12), D, RANK, 4.0) * RANK ** (-0.5)).astype(jnp.bfloat16)


def draw_factor_output(key, part):
    return (rising_draw(jax.random.fold_in(key, 13), D, RANK, 4.0) * RANK ** (-0.5)).astype(jnp.bfloat16)


def levels(rng, dims, cuts, smallest, high):
    loudness = 1.0
    for dim, parts in cuts:
        heights = jax.random.uniform(jax.random.fold_in(jax.random.fold_in(rng, 6), dim), (parts,), jnp.float32, smallest / len(cuts), high / len(cuts))
        loudness = loudness * jnp.repeat(jnp.exp(heights), dims[dim] // parts).reshape((-1,) + (1,) * (len(dims) - 1 - dim))
    return loudness


def normal_values(stream_key, dims, scale, reach, split=(), kind=jnp.bfloat16):
    result = scale * jax.random.normal(stream_key, dims, jnp.float32)
    if split:
        result = result * levels(stream_key, dims, split, -0.22, 0.18)
    return jnp.clip(result, -reach, reach).astype(kind)


def setup_inputs(seed: int = 0) -> dict:
    keys = jax.random.split(jax.random.key(seed), 16)
    first_map = normal_values(keys[0], (TOKENS, HV), 1.0, 6.0, ((0, 32), (1, 4)))
    second_map = normal_values(keys[1], (TOKENS, HV), 1.0, 6.0, ((0, 32), (1, 4)))
    lambda_head = jnp.clip(0.3 + 0.5 * jax.random.uniform(keys[2], (HEADS,), jnp.float32) ** levels(keys[2], (HEADS,), ((0, 4),), -0.2, 0.2), 0.3, 0.8)
    head_gain = jnp.clip(1.0 + 0.18 * jax.random.normal(keys[3], (HV,), jnp.float32), 0.1, 1.9)
    cot_output = normal_values(keys[4], (TOKENS, D), 1.0, 6.0, ((0, 32),))
    layer_input = normal_values(keys[5], (TOKENS, D), 1.0, 6.0, ((0, 32),))
    cot_values = draw_cot_values(jax.random.fold_in(keys[15], 71), 0)
    factor_value = draw_factor_value(jax.random.fold_in(keys[15], 71), 0)
    factor_output = draw_factor_output(jax.random.fold_in(keys[15], 71), 0)
    weight_value = normal_values(keys[9], (D, HV), 1.0, 6.0, ((0, 32), (1, 4)), jnp.float32)
    weight_output = normal_values(keys[10], (HV, D), 1.0, 6.0, ((0, 4), (1, 32)), jnp.float32)
    first_value = normal_values(keys[11], (RANK, HV), 1.0, 6.0, ((0, 32), (1, 4)), jnp.float32)
    second_value = jnp.clip(jnp.exp(math.log(1.0) - 2.9957323 * jax.random.uniform(keys[12], (RANK, HV), jnp.float32) ** levels(keys[12], (RANK, HV), ((0, 32), (1, 4)), -0.2, 0.2)), 0.05, 1.0)
    first_output = normal_values(keys[13], (RANK, HV), 1.0, 6.0, ((0, 32), (1, 4)), jnp.float32)
    second_output = jnp.clip(jnp.exp(math.log(1.0) - 2.9957323 * jax.random.uniform(keys[14], (RANK, HV), jnp.float32) ** levels(keys[14], (RANK, HV), ((0, 32), (1, 4)), -0.2, 0.2)), 0.05, 1.0)
    return dict(first_map=first_map, second_map=second_map, lambda_head=lambda_head, head_gain=head_gain, cot_output=cot_output, layer_input=layer_input, cot_values=cot_values, factor_value=factor_value, factor_output=factor_output, weight_value=weight_value, weight_output=weight_output, first_value=first_value, second_value=second_value, first_output=first_output, second_output=second_output)


norm_epsilon = 1e-06
first_decay = 0.9
second_decay = 0.95
learn_rate = 0.1

def head_output(first_map, second_map, lambda_head, head_gain):
    heads_here = lambda_head.shape[0]
    head_width = first_map.shape[1] // heads_here
    count_rows = first_map.shape[0]
    spread = jnp.repeat(lambda_head, head_width)
    differ = first_map.astype(jnp.float32) - spread[None, :] * second_map.astype(jnp.float32)
    grouped = differ.reshape(count_rows, heads_here, head_width)
    scaled = grouped * lax.rsqrt(lax.optimization_barrier(jnp.mean(grouped * grouped, -1, keepdims=True)) + norm_epsilon)
    return (scaled.reshape(count_rows, heads_here * head_width) * head_gain[None, :]).astype(jnp.bfloat16)

def moments(projected, clip_factor, first_old, second_old):
    scaled = clip_factor * projected
    first_new = first_decay * first_old + (1.0 - first_decay) * scaled
    second_new = second_decay * second_old + (1.0 - second_decay) * scaled * scaled
    return (first_new, second_new, first_new * lax.rsqrt(second_new))

def reference(first_map, second_map, lambda_head, head_gain, cot_output, layer_input, cot_values, factor_value, factor_output, weight_value, weight_output, first_value, second_value, first_output, second_output):
    heads_out = head_output(first_map, second_map, lambda_head, head_gain)
    mapped_value = jnp.dot(layer_input.astype(jnp.float32), factor_value.astype(jnp.float32), precision=lax.Precision.HIGHEST)
    mapped_output = jnp.dot(cot_output.astype(jnp.float32), factor_output.astype(jnp.float32), precision=lax.Precision.HIGHEST)
    low_value = jnp.dot(mapped_value.T, cot_values.astype(jnp.float32), precision=lax.Precision.HIGHEST)
    low_output = jnp.dot(mapped_output.T, heads_out.astype(jnp.float32), precision=lax.Precision.HIGHEST)
    total = jnp.sum(low_value * low_value) + jnp.sum(low_output * low_output)
    clip_factor = jnp.minimum(1.0, math.sqrt(RANK * HV) * lax.rsqrt(total + norm_epsilon))
    first_v, second_v, ratio_value = moments(low_value, clip_factor, first_value, second_value)
    first_o, second_o, ratio_output = moments(low_output, clip_factor, first_output, second_output)
    update_value = jnp.dot(factor_value.astype(jnp.float32), ratio_value, precision=lax.Precision.HIGHEST)
    update_output = lax.dot_general(ratio_output, factor_output.astype(jnp.float32), (((0,), (1,)), ((), ())), precision=lax.Precision.HIGHEST)
    new_value = weight_value - learn_rate * update_value
    new_output = weight_output - learn_rate * update_output
    return (new_value, first_v, second_v, new_value.astype(jnp.bfloat16), new_output, first_o, second_o, new_output.astype(jnp.bfloat16))
```

```python
import math

import jax
import jax.numpy as jnp
from jax import lax
from jax.experimental import pallas as pl
from jax.experimental.pallas import tpu as pltpu
from jax.sharding import Mesh
from jax.sharding import PartitionSpec as P

MESH = pl.DeviceIdType.MESH
RANK = 256
HV = 2048
FS = ("z", "y", "c")

norm_epsilon = 1e-06
first_decay = 0.9
second_decay = 0.95
learn_rate = 0.1

ROWS = 768
WIDE = 4096
COLS = 512
HEADS_HERE = 4
CHIPS = 16

f32 = jnp.float32
bf16 = jnp.bfloat16


def split_dot(left, right, dims):
    high = right.astype(bf16)
    low = (right - high.astype(f32)).astype(bf16)
    return lax.dot_general(left, high, dims, preferred_element_type=f32) + lax.dot_general(
        left, low, dims, preferred_element_type=f32
    )


def step_kernel(
    first_map, second_map, lambda_head, head_gain, cot_output, layer_input, cot_values,
    factor_value, factor_output, weight_value, weight_output,
    first_value, second_value, first_output, second_output,
    new_value, new_output, moved, copy_value, copy_output,
    maps, lam, gain, wide, cots, heads, factors, weights_v, weights_o, old,
    acc, lows, pair_in, summed, cross_in, squares, cross_sq, last_sq, ratios,
    load_sem, send_sem, recv_sem, pass_sem, pair_sem, cross_sem, sq_sem, last_sem,
):
    z, y, c, x = (lax.axis_index(a) for a in ("z", "y", "c", "x"))
    own = 4 * z + y
    partner = (z, y, 1 - c, x)

    def near(z_by, y_by, c_by, x_by):
        return (
            lax.rem(z + z_by, 4), lax.rem(y + y_by, 4), lax.rem(c + c_by, 2), lax.rem(x + x_by, 4)
        )

    def place(da, db, core):
        da, db = da % 4, db % 4
        return 4 * lax.rem(z + da * core + db * (1 - core), 4) + lax.rem(
            y + da * (1 - core) + db * core, 4
        )

    def chip_at(da, db):
        return near(da * c + db * (1 - c), da * (1 - c) + db * c, 0, 0)

    def load(k, source, target):
        copy = pltpu.make_async_copy(source, target, load_sem.at[k])
        copy.start()
        return copy

    own_factors = [
        load(0, factor_value, factors.at[0, own, c]),
        load(1, factor_output, factors.at[1, own, c]),
    ]
    barrier = pltpu.get_barrier_semaphore()
    greeted = [chip_at(1, 0), chip_at(3, 0), chip_at(0, 1), chip_at(0, 3), partner]
    greeted += [near(0, 0, dc, dx) for dx in (1, 2, 3) for dc in (0, 1)]
    for device in greeted:
        pl.semaphore_signal(barrier, inc=1, device_id=device, device_id_type=MESH)
    load_maps = [
        load(2, first_map, maps.at[0]),
        load(3, second_map, maps.at[1]),
        load(4, lambda_head, lam),
        load(5, head_gain, gain),
    ]
    load_wide = [load(6, layer_input, wide.at[0]), load(7, cot_output, wide.at[1])]
    load_rest = [
        load(8, cot_values, cots),
        load(9, weight_value, weights_v),
        load(10, weight_output, weights_o),
        load(11, first_value, old.at[0]),
        load(12, second_value, old.at[1]),
        load(13, first_output, old.at[2]),
        load(14, second_output, old.at[3]),
    ]
    for copy in own_factors:
        copy.wait()
    pl.semaphore_wait(barrier, len(greeted))

    class Gather:
        def __init__(self, stage, half):
            self.stage, self.half, self.sent = stage, half, []

        def fire(self, h, da, db, way):
            block = self.half(h, place(da, db, c), c)
            k = len(self.sent)
            ra, rb = da % 4, db % 4
            if way == "d":
                device, arrived = partner, pass_sem.at[self.stage, h, 4 * ra + rb]
            else:
                by = 1 if way[1] == "+" else 3
                if way[0] == "a":
                    device, ra = chip_at(by, 0), (ra - by) % 4
                else:
                    device, rb = chip_at(0, by), (rb - by) % 4
                arrived = recv_sem.at[self.stage, h, 4 * ra + rb]
            copy = pltpu.make_async_remote_copy(
                block, block, send_sem.at[k], arrived, device_id=device, device_id_type=MESH
            )
            copy.start()
            self.sent.append(copy)

        def start(self, h):
            for way in ("a+", "a-", "b+", "b-", "d"):
                self.fire(h, 0, 0, way)

        def wait(self, h, da, db):
            block = self.half(h, place(da, db, c), c)
            pltpu.make_async_remote_copy(
                block, block, send_sem.at[0], recv_sem.at[self.stage, h, 4 * (da % 4) + db % 4],
                device_id=partner, device_id_type=MESH,
            ).wait_recv()

        def take(self, h, da, db):
            self.wait(h, da, db)
            if db % 4 == 0:
                if da % 4 == 3 and h == 0:
                    self.fire(h, da, db, "a+")
                if da % 4 == 1 and h == 1:
                    self.fire(h, da, db, "a-")
                self.fire(h, da, db, "b+")
                self.fire(h, da, db, "b-")
            if db % 4 == 3 and h == 0:
                self.fire(h, da, db, "b+")
            if db % 4 == 1 and h == 1:
                self.fire(h, da, db, "b-")
            self.fire(h, da, db, "d")

        def take_all(self, places):
            for da, db in places:
                for h in (0, 1):
                    self.take(h, da, db)

        def wait_across(self, places):
            for da, db in places:
                for h in (0, 1):
                    block = self.half(h, place(da, db, 1 - c), 1 - c)
                    pltpu.make_async_remote_copy(
                        block, block, send_sem.at[0],
                        pass_sem.at[self.stage, h, 4 * (da % 4) + db % 4],
                        device_id=partner, device_id_type=MESH,
                    ).wait_recv()

        def wait_sent(self):
            for copy in self.sent:
                copy.wait_send()

    LEVELS = (
        ((0, 0),),
        ((3, 0), (1, 0), (0, 3), (0, 1)),
        ((2, 0), (3, 3), (3, 1), (1, 3), (1, 1), (0, 2)),
        ((2, 3), (2, 1), (3, 2), (1, 2)),
        ((2, 2),),
    )

    gather = Gather(0, lambda h, p, core: factors.at[h, p, core])
    gather.start(0)
    gather.start(1)

    for copy in load_maps:
        copy.wait()
    width = COLS // HEADS_HERE
    for h in range(HEADS_HERE):
        span = pl.ds(h * width, width)
        differ = maps[0, :, span].astype(f32) - lam[h] * maps[1, :, span].astype(f32)
        mean = jnp.sum(differ * differ, axis=-1, keepdims=True) * (1.0 / width)
        scaled = differ * lax.rsqrt(mean + norm_epsilon)
        heads[:, span] = (scaled * gain[span][None, :]).astype(bf16)

    def project(p, fresh):
        columns = pl.ds(pl.multiple_of(p * 256, 256), 256)
        for m in (0, 1):
            part = jnp.dot(
                wide[m, :, columns], factors[m, p].reshape(256, RANK), preferred_element_type=f32
            )
            acc[m] = part if fresh else acc[m] + part

    def at(dz, dy):
        return 4 * lax.rem(z + dz, 4) + lax.rem(y + dy, 4)

    def project_some(count, where):
        def body(i, carry):
            project(at(*where(i)), False)
            return carry

        lax.fori_loop(0, count, body, 0)

    gather.take_all(LEVELS[1])
    for copy in load_wide:
        copy.wait()
    gather.wait_across(LEVELS[0])
    project(own, True)
    gather.take_all(LEVELS[2])
    gather.wait_across(LEVELS[1])
    project_some(4, lambda i: ((1 - i // 2) * (1 + 2 * (i % 2)), (i // 2) * (1 + 2 * (i % 2))))
    gather.take_all(LEVELS[3])
    gather.wait_across(LEVELS[2])
    project_some(2, lambda i: (2 * (1 - i), 2 * i))
    project_some(4, lambda i: (1 + 2 * (i // 2), 1 + 2 * (i % 2)))
    gather.wait_across(LEVELS[3])
    project_some(
        4,
        lambda i: (
            (1 - i // 2) * 2 + (i // 2) * (1 + 2 * (i % 2)),
            (1 - i // 2) * (1 + 2 * (i % 2)) + (i // 2) * 2,
        ),
    )
    gather.take_all(LEVELS[4])
    gather.wait_across(LEVELS[4])
    project(at(2, 2), False)

    for copy in load_rest:
        copy.wait()
    pair = []
    for m in (0, 1):
        turned = acc[m].T
        high = turned.astype(bf16)
        low = (turned - high.astype(f32)).astype(bf16)
        right = (cots if m == 0 else heads)[...]
        product = jnp.dot(high, right, preferred_element_type=f32) + jnp.dot(
            low, right, preferred_element_type=f32
        )
        product = product.reshape(CHIPS, 2, 8, COLS)
        for core in (0, 1):
            lows[core, m] = product[:, core]
        copy = pltpu.make_async_remote_copy(
            lows.at[1 - c, m], pair_in.at[m], pair_sem.at[0, m], pair_sem.at[1, m],
            device_id=partner, device_id_type=MESH,
        )
        copy.start()
        pair.append(copy)
    gather.wait_sent()
    for m in (0, 1):
        pair[m].wait_recv()
        summed[:, m] = lows[c, m] + pair_in[m]
    for copy in pair:
        copy.wait_send()

    offsets = sorted(
        ((dz, dy) for dz in range(4) for dy in range(4) if (dz, dy) != (0, 0)),
        key=lambda o: -(min(o[0], 4 - o[0]) + min(o[1], 4 - o[1])),
    )
    cross = []
    for k, (dz, dy) in enumerate(offsets):
        copy = pltpu.make_async_remote_copy(
            summed.at[at(dz, dy)], cross_in.at[k], cross_sem.at[0, k], cross_sem.at[1, k],
            device_id=near(dz, dy, 0, 0), device_id_type=MESH,
        )
        copy.start()
        cross.append(copy)
    total = summed[own]
    for k in reversed(range(len(cross))):
        cross[k].wait_recv()
        total = total + cross_in[k]

    def fold(value):
        value = value.reshape(-1, 8, COLS)
        value = jnp.sum(value, axis=0)
        return sum(value[:, 128 * j : 128 * (j + 1)] for j in range(COLS // 128))

    squares[0] = fold(total * total)
    sent = []
    for k, (dz, dy) in enumerate(offsets):
        copy = pltpu.make_async_remote_copy(
            squares.at[0], cross_sq.at[k], sq_sem.at[0, k], sq_sem.at[1, k],
            device_id=near(dz, dy, 0, 0), device_id_type=MESH,
        )
        copy.start()
        sent.append(copy)
    for copy in cross:
        copy.wait_send()
    plane = squares[0]
    for k in reversed(range(len(sent))):
        sent[k].wait_recv()
        plane = plane + cross_sq[k]
    squares[1] = plane
    last = []
    for k, (dx, dc) in enumerate(((2, 1), (1, 1), (3, 1), (2, 0), (1, 0), (3, 0), (0, 1))):
        copy = pltpu.make_async_remote_copy(
            squares.at[1], last_sq.at[k], last_sem.at[0, k], last_sem.at[1, k],
            device_id=near(0, 0, dc, dx), device_id_type=MESH,
        )
        copy.start()
        last.append(copy)
    for copy in sent:
        copy.wait_send()
    whole = squares[1]
    for k in reversed(range(len(last))):
        last[k].wait_recv()
        whole = whole + last_sq[k]
    for copy in last:
        copy.wait_send()
    square_sum = jnp.sum(jnp.sum(whole, axis=1, keepdims=True), axis=0, keepdims=True)
    clip = jnp.minimum(1.0, math.sqrt(RANK * HV) * lax.rsqrt(square_sum + norm_epsilon))

    for m in (0, 1):
        scaled = clip * total[m]
        first_new = first_decay * old[2 * m] + (1.0 - first_decay) * scaled
        second_new = second_decay * old[2 * m + 1] + (1.0 - second_decay) * scaled * scaled
        moved[2 * m] = first_new
        moved[2 * m + 1] = second_new
        ratios[m, own, c] = first_new * lax.rsqrt(second_new)
    gather = Gather(1, lambda h, p, core: ratios.at[h, p, core])
    gather.start(0)
    gather.start(1)
    for level in LEVELS[1:]:
        gather.take_all(level)
    for level in LEVELS:
        gather.wait_across(level)
    gather.wait_sent()

    spread = Gather(
        2,
        lambda h, p, core: copy_value.at[p, core] if h == 0 else copy_output.at[p, core],
    )
    plain = (((1,), (0,)), ((), ()))
    added = split_dot(factors[0, own, c], ratios[0].reshape(RANK, COLS), plain)
    fresh = weights_v[...] - learn_rate * added
    copy_value[own, c] = fresh.astype(bf16)
    spread.start(0)
    new_value[...] = fresh
    added = split_dot(factors[1, own, c], ratios[1].reshape(RANK, COLS), plain)
    fresh = weights_o[...] - learn_rate * added.T
    copy_output[own, c] = fresh.astype(bf16)
    spread.start(1)
    new_output[...] = fresh
    for level in LEVELS[1:]:
        spread.take_all(level)
    for level in LEVELS:
        spread.wait_across(level)
    spread.wait_sent()


def write_kernel(new_value, new_output, moved, copy_value, copy_output, *rest):
    outs, sem = rest[:8], rest[8]
    new_v, first_v, second_v, copy_v, new_o, first_o, second_o, copy_o = outs
    pairs = [(copy_value, copy_v)]
    pairs += [
        (copy_output.at[k], copy_o.at[:, pl.ds(128 * k, 128)]) for k in range(copy_output.shape[0])
    ]
    pairs += [(new_value, new_v), (new_output, new_o)]
    pairs += [(moved.at[k], out) for k, out in enumerate((first_v, second_v, first_o, second_o))]
    copies = [pltpu.make_async_copy(s, t, sem.at[k]) for k, (s, t) in enumerate(pairs)]
    for copy in copies:
        copy.start()
    for copy in copies:
        copy.wait()


def shards(*args):
    any_space = pl.BlockSpec(memory_space=pltpu.HBM)
    vmem = pl.BlockSpec(memory_space=pltpu.VMEM)
    dma = pltpu.SemaphoreType.DMA
    new_value, new_output, moved, copy_value, copy_output = pl.pallas_call(
        step_kernel,
        out_shape=(
            pltpu.VMEM((128, COLS), f32),
            pltpu.VMEM((COLS, 128), f32),
            pltpu.VMEM((4, 8, COLS), f32),
            pltpu.VMEM((CHIPS, 2, 128, COLS), bf16),
            pltpu.VMEM((CHIPS, 2, COLS, 128), bf16),
        ),
        in_specs=[any_space] * 15,
        out_specs=(vmem,) * 5,
        scratch_shapes=[
            pltpu.VMEM((2, ROWS, COLS), bf16),
            pltpu.SMEM((HEADS_HERE,), f32),
            pltpu.VMEM((COLS,), f32),
            pltpu.VMEM((2, ROWS, WIDE), bf16),
            pltpu.VMEM((ROWS, COLS), bf16),
            pltpu.VMEM((ROWS, COLS), bf16),
            pltpu.VMEM((2, CHIPS, 2, 128, RANK), bf16),
            pltpu.VMEM((128, COLS), f32),
            pltpu.VMEM((COLS, 128), f32),
            pltpu.VMEM((4, 8, COLS), f32),
            pltpu.VMEM((2, ROWS, RANK), f32),
            pltpu.VMEM((2, 2, CHIPS, 8, COLS), f32),
            pltpu.VMEM((2, CHIPS, 8, COLS), f32),
            pltpu.VMEM((CHIPS, 2, 8, COLS), f32),
            pltpu.VMEM((15, 2, 8, COLS), f32),
            pltpu.VMEM((2, 8, 128), f32),
            pltpu.VMEM((15, 8, 128), f32),
            pltpu.VMEM((7, 8, 128), f32),
            pltpu.VMEM((2, CHIPS, 2, 8, COLS), f32),
            dma((15,)),
            dma((64,)),
            dma((3, 2, 16)),
            dma((3, 2, 16)),
            dma((2, 2)),
            dma((2, 15)),
            dma((2, 15)),
            dma((2, 7)),
        ],
        compiler_params=pltpu.CompilerParams(
            collective_id=0, has_side_effects=True, vmem_limit_bytes=46 * 1024 * 1024
        ),
        name="step",
    )(*args)
    return pl.pallas_call(
        write_kernel,
        out_shape=(
            jax.ShapeDtypeStruct((128, COLS), f32),
            jax.ShapeDtypeStruct((8, COLS), f32),
            jax.ShapeDtypeStruct((8, COLS), f32),
            jax.ShapeDtypeStruct((WIDE, COLS), bf16),
            jax.ShapeDtypeStruct((COLS, 128), f32),
            jax.ShapeDtypeStruct((8, COLS), f32),
            jax.ShapeDtypeStruct((8, COLS), f32),
            jax.ShapeDtypeStruct((COLS, WIDE), bf16),
        ),
        in_specs=[vmem] * 5,
        out_specs=(any_space,) * 8,
        scratch_shapes=[dma((2 * CHIPS + 7,))],
        compiler_params=pltpu.CompilerParams(vmem_limit_bytes=4 * 1024 * 1024),
        name="write",
    )(
        new_value,
        new_output,
        moved,
        copy_value.reshape(WIDE, COLS),
        copy_output.reshape(2 * CHIPS, COLS, 128),
    )


def solution(mesh):
    torus = Mesh(mesh.devices.reshape(4, 4, 2, 4), ("z", "y", "c", "x"))
    split = P(FS, "x")
    whole = P(FS, None)
    return jax.shard_map(
        shards,
        mesh=torus,
        in_specs=(
            split, split, P("x"), P("x"), whole, whole, split, whole, whole,
            split, P("x", FS), split, split, split, split,
        ),
        out_specs=(
            split, split, split, P(None, "x"), P("x", FS), split, split, P("x", None),
        ),
        check_vma=False,
    )
```

```python
import math

import jax
import jax.numpy as jnp
from jax import lax
from jax.experimental import pallas as pl
from jax.experimental.pallas import tpu as pltpu
from jax.sharding import Mesh
from jax.sharding import PartitionSpec as P

MESH = pl.DeviceIdType.MESH
RANK = 256
HV = 2048
FS = ("z", "y", "c")

norm_epsilon = 1e-06
first_decay = 0.9
second_decay = 0.95
learn_rate = 0.1

ROWS = 768
WIDE = 4096
COLS = 512
HEADS_HERE = 4
CHIPS = 16

f32 = jnp.float32
bf16 = jnp.bfloat16


def step_kernel(
    first_map, second_map, lambda_head, head_gain, cot_output, layer_input, cot_values,
    factor_value, factor_output, weight_value, weight_output,
    first_value, second_value, first_output, second_output,
    new_value, new_output, moved, copy_value, copy_output,
    maps, lam, gain, wide, cots, heads, factors, weights_v, weights_o, moments,
    acc, lows, pair_in, summed, cross_in, squares, cross_sq, last_sq, low_all, ratios,
    load_sem, send_sem, recv_sem, pass_sem, pair_sem, cross_sem, sq_sem, low_sem, low_pass,
):
    z, y, c, x = (lax.axis_index(a) for a in ("z", "y", "c", "x"))
    own = 4 * z + y
    mine = 2 * own + c
    partner = (z, y, 1 - c, x)

    def near(z_by, y_by, c_by, x_by):
        return (
            lax.rem(z + z_by, 4), lax.rem(y + y_by, 4), lax.rem(c + c_by, 2), lax.rem(x + x_by, 4)
        )

    def at(dz, dy):
        return 4 * lax.rem(z + dz, 4) + lax.rem(y + dy, 4)

    def place(da, db, core):
        return at(da * core + db * (1 - core), da * (1 - core) + db * core)

    def chip_at(da, db):
        return near(da * c + db * (1 - c), da * (1 - c) + db * c, 0, 0)

    def remote(source, target, sent, arrived, device):
        return pltpu.make_async_remote_copy(
            source, target, sent, arrived, device_id=device, device_id_type=MESH
        )

    def arrive(block, semaphore):
        remote(block, block, send_sem.at[0, 0], semaphore, partner).wait_recv()

    def sent_off(block, semaphore):
        remote(block, block, semaphore, recv_sem.at[0, 0, 0], partner).wait_send()

    def load(k, source, target):
        copy = pltpu.make_async_copy(source, target, load_sem.at[k])
        copy.start()
        return copy

    own_factors = [
        load(0, factor_value, factors.at[0, mine]),
        load(1, factor_output, factors.at[1, mine]),
    ]
    barrier = pltpu.get_barrier_semaphore()
    greeted = [chip_at(1, 0), chip_at(3, 0), chip_at(0, 1), chip_at(0, 3), partner]
    greeted += [near(0, 0, dc, dx) for dx in (1, 2, 3) for dc in (0, 1)]
    for device in greeted:
        pl.semaphore_signal(barrier, inc=1, device_id=device, device_id_type=MESH)
    load_maps = [
        load(2, first_map, maps.at[0]),
        load(3, second_map, maps.at[1]),
        load(4, lambda_head, lam),
        load(5, head_gain, gain),
    ]
    load_wide = [load(6, layer_input, wide.at[0]), load(7, cot_output, wide.at[1])]
    load_moments = [
        load(8, first_value, moments.at[0, mine, 0]),
        load(9, second_value, moments.at[0, mine, 1]),
        load(10, first_output, moments.at[1, mine, 0]),
        load(11, second_output, moments.at[1, mine, 1]),
    ]
    load_rest = [
        load(12, cot_values, cots),
        load(13, weight_value, weights_v),
        load(14, weight_output, weights_o),
    ]
    for copy in own_factors:
        copy.wait()
    pl.semaphore_wait(barrier, len(greeted))

    LEVELS = (
        ((0, 0),),
        ((3, 0), (1, 0), (0, 3), (0, 1)),
        ((2, 0), (3, 3), (3, 1), (1, 3), (1, 1), (0, 2)),
        ((2, 3), (2, 1), (3, 2), (1, 2)),
        ((2, 2),),
    )

    class Gather:
        def __init__(self, stage, arrivals, halves):
            self.halves, self.counts = halves, [0, 0]
            self.sent = [send_sem.at[stage, h] for h in (0, 1)]
            self.arrived = recv_sem.at[arrivals]
            self.passed = pass_sem.at[stage]

        def fire(self, h, da, db, way):
            block = self.halves[h].at[2 * place(da, db, c) + c]
            if way == "d":
                level = min(da, 4 - da) + min(db, 4 - db)
                device, arrived = partner, self.passed.at[h, level]
            else:
                by = 1 if way[1] == "+" else 3
                if way[0] == "a":
                    device, da = chip_at(by, 0), (da - by) % 4
                else:
                    device, db = chip_at(0, by), (db - by) % 4
                arrived = self.arrived.at[h, 4 * da + db]
            remote(block, block, self.sent[h], arrived, device).start()
            self.counts[h] += 1

        def start(self, h):
            for way in ("b+", "b-", "a+", "a-", "d"):
                self.fire(h, 0, 0, way)

        def take(self, h, da, db):
            arrive(self.halves[h].at[2 * place(da, db, c) + c], self.arrived.at[h, 4 * da + db])
            if db == 0:
                if da == 3 and h == 0:
                    self.fire(h, da, db, "a+")
                if da == 1 and h == 1:
                    self.fire(h, da, db, "a-")
                self.fire(h, da, db, "b+")
                self.fire(h, da, db, "b-")
            if db == 3 and h == 0:
                self.fire(h, da, db, "b+")
            if db == 1 and h == 1:
                self.fire(h, da, db, "b-")
            self.fire(h, da, db, "d")

        def take_level(self, level, halves=(0, 1)):
            for h in halves:
                for da, db in LEVELS[level]:
                    self.take(h, da, db)

        def across(self, level):
            for h in (0, 1):
                arrive(self.halves[h].at[pl.ds(0, len(LEVELS[level]))], self.passed.at[h, level])

        def finish(self):
            for h in (0, 1):
                sent_off(self.halves[h].at[pl.ds(0, self.counts[h])], self.sent[h])

    gather = Gather(0, 0, (factors.at[0], factors.at[1]))
    gather.start(0)
    gather.start(1)

    for copy in load_maps:
        copy.wait()
    width = COLS // HEADS_HERE
    for h in range(HEADS_HERE):
        span = pl.ds(h * width, width)
        differ = maps[0, :, span].astype(f32) - lam[h] * maps[1, :, span].astype(f32)
        mean = jnp.sum(differ * differ, axis=-1, keepdims=True) * (1.0 / width)
        scaled = differ * lax.rsqrt(mean + norm_epsilon)
        heads[:, span] = (scaled * gain[span][None, :]).astype(bf16)

    def project(*chips, fresh=False):
        for m in (0, 1):
            left = [
                wide[m, :, pl.ds(pl.multiple_of(p * 256, 256), 256)]
                for p in chips
            ]
            right = [factors[m, pl.ds(2 * p, 2)].reshape(256, RANK) for p in chips]
            if len(chips) > 1:
                left, right = [jnp.concatenate(left, axis=1)], [jnp.concatenate(right, axis=0)]
            part = jnp.dot(left[0], right[0], preferred_element_type=f32)
            acc[m] = part if fresh else acc[m] + part

    gather.take_level(1)
    for copy in load_wide:
        copy.wait()
    gather.across(0)
    project(own, fresh=True)
    gather.take_level(2, (0,))
    gather.across(1)
    project(at(1, 0), at(3, 0))
    gather.take_level(2, (1,))
    project(at(0, 1), at(0, 3))
    gather.take_level(3, (0,))
    gather.across(2)
    project(at(2, 0), at(0, 2))
    gather.take_level(3, (1,))
    project(at(1, 1), at(3, 3))
    gather.take_level(4)
    for copy in load_moments:
        copy.wait()
    moment_gather = Gather(1, 1, (moments.at[0], moments.at[1]))
    moment_gather.start(0)
    moment_gather.start(1)
    project(at(1, 3), at(3, 1))
    gather.across(3)
    project(at(2, 1), at(2, 3))
    project(at(1, 2), at(3, 2))
    gather.across(4)
    project(at(2, 2))

    for copy in load_rest:
        copy.wait()
    pair = []
    for m in (0, 1):
        turned = acc[m].T
        high = turned.astype(bf16)
        low = (turned - high.astype(f32)).astype(bf16)
        right = (cots if m == 0 else heads)[...]
        product = jnp.dot(high, right, preferred_element_type=f32) + jnp.dot(
            low, right, preferred_element_type=f32
        )
        product = product.reshape(CHIPS, 2, 8, COLS)
        for core in (0, 1):
            lows[core, m] = product[:, core]
        copy = remote(
            lows.at[1 - c, m], pair_in.at[m], pair_sem.at[0, m], pair_sem.at[1, m], partner
        )
        copy.start()
        pair.append(copy)
    moment_gather.take_level(1)

    offsets = sorted(
        ((dz, dy) for dz in range(4) for dy in range(4) if (dz, dy) != (0, 0)),
        key=lambda o: -(min(o[0], 4 - o[0]) + min(o[1], 4 - o[1])),
    )
    for m in (0, 1):
        pair[m].wait_recv()
        summed[m] = lows[c, m] + pair_in[m]
        for k, (dz, dy) in enumerate(offsets):
            remote(
                summed.at[m, at(dz, dy)], cross_in.at[m, k], cross_sem.at[0, m], cross_sem.at[1, m],
                near(dz, dy, 0, 0),
            ).start()
    moment_gather.take_level(2)
    totals = []
    for m in (0, 1):
        arrive(cross_in.at[m], cross_sem.at[1, m])
        total = summed[m, own]
        for k in range(len(offsets)):
            total = total + cross_in[m, k]
        low_all[mine, m] = total
        totals.append(total)

    def fold(value):
        return sum(value[:, 128 * j : 128 * (j + 1)] for j in range(COLS // 128))

    squares[0] = fold(totals[0] * totals[0] + totals[1] * totals[1])
    for k, (dz, dy) in enumerate(offsets):
        remote(
            squares.at[0], cross_sq.at[k], sq_sem.at[0, 0], sq_sem.at[0, 1], near(dz, dy, 0, 0)
        ).start()
    block = low_all.at[mine]
    for k, (dz, dy) in enumerate(offsets):
        remote(block, block, low_sem.at[15], low_sem.at[k], near(dz, dy, 0, 0)).start()
    remote(block, block, low_pass.at[0], low_pass.at[1], partner).start()
    moment_gather.take_level(3)
    arrive(cross_sq, sq_sem.at[0, 1])
    plane = squares[0]
    for k in range(len(offsets)):
        plane = plane + cross_sq[k]
    squares[1] = plane
    for k, (dx, dc) in enumerate(((2, 1), (1, 1), (3, 1), (2, 0), (1, 0), (3, 0), (0, 1))):
        remote(
            squares.at[1], last_sq.at[k], sq_sem.at[1, 0], sq_sem.at[1, 1], near(0, 0, dc, dx)
        ).start()
    moment_gather.take_level(4)
    for k, (dz, dy) in reversed(list(enumerate(offsets))):
        block = low_all.at[2 * at((-dz) % 4, (-dy) % 4) + c]
        arrive(block, low_sem.at[k])
        remote(block, block, low_pass.at[0], low_pass.at[1], partner).start()
    arrive(last_sq, sq_sem.at[1, 1])
    whole = squares[1]
    for k in range(7):
        whole = whole + last_sq[k]
    square_sum = jnp.sum(jnp.sum(whole, axis=1, keepdims=True), axis=0, keepdims=True)
    clip = jnp.minimum(1.0, math.sqrt(RANK * HV) * lax.rsqrt(square_sum + norm_epsilon))
    for level in range(5):
        moment_gather.across(level)
    arrive(low_all.at[pl.ds(0, CHIPS)], low_pass.at[1])

    def moved_by(low, first_old, second_old):
        scaled = clip * low
        first_new = first_decay * first_old + (1.0 - first_decay) * scaled
        second_new = second_decay * second_old + (1.0 - second_decay) * scaled * scaled
        return first_new, second_new

    def added(m):
        step = 4
        for k in range(0, 2 * CHIPS, step):
            low = low_all[k : k + step, m].reshape(8 * step, COLS)
            first_old = moments[m, k : k + step, 0].reshape(8 * step, COLS)
            second_old = moments[m, k : k + step, 1].reshape(8 * step, COLS)
            first_new, second_new = moved_by(low, first_old, second_old)
            ratio = first_new * lax.rsqrt(second_new)
            high = ratio.astype(bf16)
            ratios[m, 0, 8 * k : 8 * (k + step)] = high
            ratios[m, 1, 8 * k : 8 * (k + step)] = (ratio - high.astype(f32)).astype(bf16)
        left = factors[m, mine]
        return jnp.dot(left, ratios[m, 0], preferred_element_type=f32) + jnp.dot(
            left, ratios[m, 1], preferred_element_type=f32
        )

    spread = Gather(2, 0, (copy_value, copy_output))
    fresh = weights_v[...] - learn_rate * added(0)
    copy_value[mine] = fresh.astype(bf16)
    spread.start(0)
    new_value[...] = fresh
    fresh = weights_o[...] - learn_rate * added(1).T
    copy_output[mine] = fresh.astype(bf16)
    spread.start(1)
    new_output[...] = fresh
    for m in (0, 1):
        first_new, second_new = moved_by(
            low_all[mine, m], moments[m, mine, 0], moments[m, mine, 1]
        )
        moved[2 * m] = first_new
        moved[2 * m + 1] = second_new
    gather.finish()
    moment_gather.finish()
    for copy in pair:
        copy.wait_send()
    for m in (0, 1):
        sent_off(cross_in.at[m], cross_sem.at[0, m])
    sent_off(cross_sq, sq_sem.at[0, 0])
    sent_off(last_sq, sq_sem.at[1, 0])
    sent_off(low_all.at[pl.ds(0, 15)], low_sem.at[15])
    sent_off(low_all.at[pl.ds(0, CHIPS)], low_pass.at[0])
    for level in (1, 2, 3, 4):
        spread.take_level(level)
    for level in range(5):
        spread.across(level)
    spread.finish()


def write_kernel(new_value, new_output, moved, copy_value, copy_output, *rest):
    outs, sem = rest[:8], rest[8]
    new_v, first_v, second_v, copy_v, new_o, first_o, second_o, copy_o = outs
    pairs = [(copy_value, copy_v)]
    pairs += [
        (copy_output.at[k], copy_o.at[:, pl.ds(128 * k, 128)]) for k in range(copy_output.shape[0])
    ]
    pairs += [(new_value, new_v), (new_output, new_o)]
    pairs += [(moved.at[k], out) for k, out in enumerate((first_v, second_v, first_o, second_o))]
    copies = [pltpu.make_async_copy(s, t, sem.at[k]) for k, (s, t) in enumerate(pairs)]
    for copy in copies:
        copy.start()
    for copy in copies:
        copy.wait()


def shards(*args):
    any_space = pl.BlockSpec(memory_space=pltpu.HBM)
    vmem = pl.BlockSpec(memory_space=pltpu.VMEM)
    dma = pltpu.SemaphoreType.DMA
    new_value, new_output, moved, copy_value, copy_output = pl.pallas_call(
        step_kernel,
        out_shape=(
            pltpu.VMEM((128, COLS), f32),
            pltpu.VMEM((COLS, 128), f32),
            pltpu.VMEM((4, 8, COLS), f32),
            pltpu.VMEM((2 * CHIPS, 128, COLS), bf16),
            pltpu.VMEM((2 * CHIPS, COLS, 128), bf16),
        ),
        in_specs=[any_space] * 15,
        out_specs=(vmem,) * 5,
        scratch_shapes=[
            pltpu.VMEM((2, ROWS, COLS), bf16),
            pltpu.SMEM((HEADS_HERE,), f32),
            pltpu.VMEM((COLS,), f32),
            pltpu.VMEM((2, ROWS, WIDE), bf16),
            pltpu.VMEM((ROWS, COLS), bf16),
            pltpu.VMEM((ROWS, COLS), bf16),
            pltpu.VMEM((2, 2 * CHIPS, 128, RANK), bf16),
            pltpu.VMEM((128, COLS), f32),
            pltpu.VMEM((COLS, 128), f32),
            pltpu.VMEM((2, 2 * CHIPS, 2, 8, COLS), f32),
            pltpu.VMEM((2, ROWS, RANK), f32),
            pltpu.VMEM((2, 2, CHIPS, 8, COLS), f32),
            pltpu.VMEM((2, CHIPS, 8, COLS), f32),
            pltpu.VMEM((2, CHIPS, 8, COLS), f32),
            pltpu.VMEM((2, 15, 8, COLS), f32),
            pltpu.VMEM((2, 8, 128), f32),
            pltpu.VMEM((15, 8, 128), f32),
            pltpu.VMEM((7, 8, 128), f32),
            pltpu.VMEM((2 * CHIPS, 2, 8, COLS), f32),
            pltpu.VMEM((2, 2, RANK, COLS), bf16),
            dma((15,)),
            dma((3, 2)),
            dma((2, 2, 16)),
            dma((3, 2, 5)),
            dma((2, 2)),
            dma((2, 2)),
            dma((2, 2)),
            dma((16,)),
            dma((2,)),
        ],
        compiler_params=pltpu.CompilerParams(
            collective_id=0, has_side_effects=True, vmem_limit_bytes=46 * 1024 * 1024
        ),
        name="step",
    )(*args)
    return pl.pallas_call(
        write_kernel,
        out_shape=(
            jax.ShapeDtypeStruct((128, COLS), f32),
            jax.ShapeDtypeStruct((8, COLS), f32),
            jax.ShapeDtypeStruct((8, COLS), f32),
            jax.ShapeDtypeStruct((WIDE, COLS), bf16),
            jax.ShapeDtypeStruct((COLS, 128), f32),
            jax.ShapeDtypeStruct((8, COLS), f32),
            jax.ShapeDtypeStruct((8, COLS), f32),
            jax.ShapeDtypeStruct((COLS, WIDE), bf16),
        ),
        in_specs=[vmem] * 5,
        out_specs=(any_space,) * 8,
        scratch_shapes=[dma((2 * CHIPS + 7,))],
        compiler_params=pltpu.CompilerParams(vmem_limit_bytes=4 * 1024 * 1024),
        name="write",
    )(
        new_value,
        new_output,
        moved,
        copy_value.reshape(WIDE, COLS),
        copy_output,
    )


def solution(mesh):
    torus = Mesh(mesh.devices.reshape(4, 4, 2, 4), ("z", "y", "c", "x"))
    split = P(FS, "x")
    whole = P(FS, None)
    return jax.shard_map(
        shards,
        mesh=torus,
        in_specs=(
            split, split, P("x"), P("x"), whole, whole, split, whole, whole,
            split, P("x", FS), split, split, split, split,
        ),
        out_specs=(
            split, split, split, P(None, "x"), P("x", FS), split, split, P("x", None),
        ),
        check_vma=False,
    )
```

```python
import math

import jax
import jax.numpy as jnp
from jax import lax
from jax.experimental import pallas as pl
from jax.experimental.pallas import tpu as pltpu
from jax.sharding import Mesh
from jax.sharding import PartitionSpec as P

MESH = pl.DeviceIdType.MESH
RANK = 256
HV = 2048
FS = ("z", "y", "c")

norm_epsilon = 1e-06
first_decay = 0.9
second_decay = 0.95
learn_rate = 0.1

ROWS = 768
WIDE = 4096
COLS = 512
HEADS_HERE = 4
CHIPS = 16
LANES = 128

f32 = jnp.float32
bf16 = jnp.bfloat16

LEVELS = (
    ((0, 0),),
    ((3, 0), (1, 0), (0, 3), (0, 1)),
    ((2, 0), (3, 3), (3, 1), (1, 3), (1, 1), (0, 2)),
    ((2, 3), (2, 1), (3, 2), (1, 2)),
    ((2, 2),),
)


def step_kernel(
    first_map, second_map, lambda_head, head_gain, cot_output, layer_input, cot_values,
    factor_value, factor_output, weight_value, weight_output,
    first_value, second_value, first_output, second_output,
    new_weights, moved, copies,
    maps, lam, gain, wide, rights, right_in, factors, weights, moments,
    acc, turned, summed, cross_in, squares, cross_sq, last_sq, low_all, ratios, added, back, back_moved,
    load_sem, out_sem, in_sem, send_sem, recv_sem, pass_sem, cross_sem, sq_sem, low_sem,
):
    z, y, c, x = (lax.axis_index(a) for a in ("z", "y", "c", "x"))
    own = 4 * z + y
    mine = 2 * own + c
    partner = (z, y, 1 - c, x)

    def near(z_by, y_by, c_by, x_by):
        return (
            lax.rem(z + z_by, 4), lax.rem(y + y_by, 4), lax.rem(c + c_by, 2), lax.rem(x + x_by, 4)
        )

    def at(dz, dy):
        return 4 * lax.rem(z + dz, 4) + lax.rem(y + dy, 4)

    def place(da, db):
        return at(da * c + db * (1 - c), da * (1 - c) + db * c)

    def chip_at(da, db):
        return near(da * c + db * (1 - c), da * (1 - c) + db * c, 0, 0)

    def remote(source, target, sent, arrived, device):
        return pltpu.make_async_remote_copy(
            source, target, sent, arrived, device_id=device, device_id_type=MESH
        )

    def arrive(block, semaphore):
        remote(block, block, out_sem.at[0], semaphore, partner).wait_recv()

    def sent_off(block, semaphore):
        remote(block, block, semaphore, in_sem.at[0], partner).wait_send()

    def load(k, source, target):
        copy = pltpu.make_async_copy(source, target, load_sem.at[k])
        copy.start()
        return copy

    def loaded(k, target):
        pltpu.make_async_copy(target, target, load_sem.at[k]).wait()

    value_args = (factor_value, first_value, second_value, layer_input)
    output_args = (factor_output, first_output, second_output, cot_output)

    def columns(ref, j):
        return ref.at[:, pl.ds(LANES * j, LANES)]

    def rows(ref, j):
        return ref.at[pl.ds(LANES * j, LANES)]

    def load_first(args):
        load(0, args[0], factors.at[mine])

    def load_later(args, weight, pieces):
        load(1, args[3], wide.at[0])
        load(2, args[1], moments.at[mine, 0])
        load(2, args[2], moments.at[mine, 1])
        for j in range(4):
            load(3, pieces(weight, j), rows(weights.at[c], j))

    pl.when(c == 0)(lambda: load_first(value_args))
    pl.when(c == 1)(lambda: load_first(output_args))
    barrier = pltpu.get_barrier_semaphore()
    greeted = [chip_at(1, 0), chip_at(3, 0), chip_at(0, 1), chip_at(0, 3), partner]
    greeted += [near(0, 0, dc, dx) for dx in (1, 2, 3) for dc in (0, 1)]
    for device in greeted:
        pl.semaphore_signal(barrier, inc=1, device_id=device, device_id_type=MESH)
    load_maps = [
        load(4, first_map, maps.at[0]),
        load(5, second_map, maps.at[1]),
        load(6, lambda_head, lam),
        load(7, head_gain, gain),
    ]
    pl.when(c == 0)(lambda: load_later(value_args, weight_value, columns))
    pl.when(c == 1)(lambda: load_later(output_args, weight_output, rows))
    load(8, cot_values, rights.at[0])
    pl.semaphore_wait(barrier, len(greeted))

    def hand(k, source, target):
        remote(source, target, out_sem.at[k], in_sem.at[k], partner).start()

    def hand_later(args, weight, pieces):
        hand(1, args[3], wide.at[1])
        hand(2, args[1], moments.at[mine, 0])
        hand(2, args[2], moments.at[mine, 1])
        for j in range(4):
            hand(3, pieces(weight, j), rows(weights.at[c], j))

    pl.when(c == 0)(lambda: hand(0, factor_output, factors.at[mine]))
    pl.when(c == 1)(lambda: hand(0, factor_value, factors.at[mine]))

    class Gather:
        def __init__(self, stage, arrivals, blocks, passed=None):
            self.blocks, self.passed, self.sent = blocks, passed, send_sem.at[stage]
            self.counts = [0, 0]
            self.arrived = recv_sem.at[arrivals]

        def block(self, g, da, db):
            return self.blocks.at[2 * place(da, db) + (c if g == 0 else 1 - c)]

        def fire(self, g, da, db, *ways):
            block = self.block(g, da, db)
            for way in ways:
                ra, rb = da, db
                by = 1 if way[1] == "+" else 3
                if way[0] == "a":
                    device, ra = chip_at(by, 0), (da - by) % 4
                else:
                    device, rb = chip_at(0, by), (db - by) % 4
                remote(
                    block, block, self.sent.at[g], self.arrived.at[g, 4 * ra + rb], device
                ).start()
                self.counts[g] += 1
            if self.passed is not None:
                level = min(da, 4 - da) + min(db, 4 - db)
                remote(block, block, self.sent.at[g], self.passed.at[level], partner).start()
                self.counts[g] += 1

        def start(self, g):
            self.fire(g, 0, 0, "b+", "b-", "a+", "a-")

        def take(self, g, da, db):
            arrive(self.block(g, da, db), self.arrived.at[g, 4 * da + db])
            ways = []
            if db == 0:
                if da == (3 if g == 0 else 1):
                    ways.append("a+" if g == 0 else "a-")
                ways += ["b+", "b-"]
            elif db == (3 if (da in (0, 1)) == (g == 0) else 1):
                ways.append("b+" if db == 3 else "b-")
            self.fire(g, da, db, *ways)

        def take_level(self, level, parts=(0, 1)):
            for g in parts:
                for da, db in LEVELS[level]:
                    self.take(g, da, db)

        def finish(self):
            for g in (0, 1):
                sent_off(self.blocks.at[pl.ds(0, self.counts[g])], self.sent.at[g])

    loaded(0, factors.at[mine])
    gather = Gather(0, 0, factors)
    gather.start(0)
    pl.when(c == 0)(lambda: hand_later(output_args, weight_output, rows))
    pl.when(c == 1)(lambda: hand_later(value_args, weight_value, columns))
    for copy in load_maps:
        copy.wait()
    width = COLS // HEADS_HERE
    for h in range(HEADS_HERE):
        span = pl.ds(h * width, width)
        differ = maps[0, :, span].astype(f32) - lam[h] * maps[1, :, span].astype(f32)
        mean = jnp.sum(differ * differ, axis=-1, keepdims=True) * (1.0 / width)
        scaled = differ * lax.rsqrt(mean + norm_epsilon)
        rights[1, :, span] = (scaled * gain[span][None, :]).astype(bf16)
    arrive(factors.at[mine], in_sem.at[0])
    gather.start(1)
    loaded(8, rights.at[0])
    hand(4, rights.at[1 - c], right_in)

    def project(t, *chips, fresh=False):
        left = [wide[t, :, pl.ds(pl.multiple_of(p * 256, 256), 256)] for p in chips]
        right = [factors[pl.ds(2 * p, 2)].reshape(256, RANK) for p in chips]
        if len(chips) > 1:
            left, right = [jnp.concatenate(left, axis=1)], [jnp.concatenate(right, axis=0)]
        part = jnp.dot(left[0], right[0], preferred_element_type=f32)
        acc[t] = part if fresh else acc[t] + part

    PAIRS = (
        None,
        (((1, 0), (3, 0)), ((0, 1), (0, 3))),
        (((2, 0), (0, 2)), ((1, 1), (3, 3)), ((1, 3), (3, 1))),
        (((2, 1), (2, 3)), ((1, 2), (3, 2))),
    )

    def project_pairs(t, level, *which):
        for k in which:
            (z0, y0), (z1, y1) = PAIRS[level][k]
            project(t, at(z0, y0), at(z1, y1))

    gather.take_level(1)
    loaded(1, wide.at[0])
    project(0, own, fresh=True)
    gather.take_level(2, (0,))
    project_pairs(0, 1, 0)
    gather.take_level(2, (1,))
    project_pairs(0, 1, 1)
    gather.take_level(3, (0,))
    arrive(wide.at[1], in_sem.at[1])
    project(1, own, fresh=True)
    project_pairs(1, 1, 0)
    loaded(2, moments.at[mine])
    arrive(moments.at[mine], in_sem.at[2])
    moment_gather = Gather(1, 1, moments)
    moment_gather.start(0)
    moment_gather.start(1)
    gather.take_level(3, (1,))
    project_pairs(1, 1, 1)
    project_pairs(0, 2, 0, 1, 2)
    project_pairs(1, 2, 0)
    project_pairs(1, 2, 1, 2)
    project_pairs(0, 3, 0, 1)
    gather.take_level(4)
    moment_gather.take_level(1)
    project_pairs(1, 3, 0, 1)
    for t in (0, 1):
        project(t, at(2, 2))
    arrive(right_in, in_sem.at[4])
    product = None
    for t in (0, 1):
        flat = acc[t].T
        high = flat.astype(bf16)
        turned[t, :RANK] = high
        turned[t, RANK:] = (flat - high.astype(f32)).astype(bf16)
        right = rights[c] if t == 0 else right_in[...]
        part = jnp.dot(turned[t], right, preferred_element_type=f32)
        product = part if t == 0 else product + part
    summed[...] = (product[:RANK] + product[RANK:]).reshape(CHIPS, 16, COLS)

    offsets = sorted(
        ((dz, dy) for dz in range(4) for dy in range(4) if (dz, dy) != (0, 0)),
        key=lambda o: -(min(o[0], 4 - o[0]) + min(o[1], 4 - o[1])),
    )
    for k, (dz, dy) in enumerate(offsets):
        remote(
            summed.at[at(dz, dy)], cross_in.at[k], cross_sem.at[0], cross_sem.at[1],
            near(dz, dy, 0, 0),
        ).start()
    arrive(cross_in, cross_sem.at[1])
    total = summed[own]
    for k in range(len(offsets)):
        total = total + cross_in[k]
    low_all[own] = total

    def fold(value):
        value = value[:8] + value[8:]
        return sum(value[:, LANES * j : LANES * (j + 1)] for j in range(COLS // LANES))

    squares[0] = fold(total * total)
    for k, (dz, dy) in enumerate(offsets):
        remote(
            squares.at[0], cross_sq.at[k], sq_sem.at[0, 0], sq_sem.at[0, 1], near(dz, dy, 0, 0)
        ).start()
    def send_low(block, way):
        for by in (2, 1, 3):
            device = chip_at(by, 0) if way == 0 else chip_at(0, by)
            remote(block, block, low_sem.at[way, 0], low_sem.at[way, 1], device).start()

    send_low(low_all.at[own], 0)
    send_low(low_all.at[own], 1)
    moment_gather.take_level(2)
    arrive(low_all.at[pl.ds(0, 3)], low_sem.at[0, 1])
    for k in (2, 1, 3):
        send_low(low_all.at[place(k, 0)], 1)
    arrive(cross_sq, sq_sem.at[0, 1])
    plane = squares[0]
    for k in range(len(offsets)):
        plane = plane + cross_sq[k]
    squares[1] = plane
    for k, (dx, dc) in enumerate(((2, 1), (1, 1), (3, 1), (2, 0), (1, 0), (3, 0), (0, 1))):
        remote(
            squares.at[1], last_sq.at[k], sq_sem.at[1, 0], sq_sem.at[1, 1], near(0, 0, dc, dx)
        ).start()
    moment_gather.take_level(3)
    arrive(weights.at[0], in_sem.at[3])
    loaded(3, weights.at[0])
    arrive(low_all.at[pl.ds(0, 12)], low_sem.at[1, 1])
    arrive(last_sq, sq_sem.at[1, 1])
    whole = squares[1]
    for k in range(7):
        whole = whole + last_sq[k]
    square_sum = jnp.sum(jnp.sum(whole, axis=1, keepdims=True), axis=0, keepdims=True)
    clip = jnp.minimum(1.0, math.sqrt(RANK * HV) * lax.rsqrt(square_sum + norm_epsilon))

    moment_gather.take_level(4)
    def moved_by(low, first_old, second_old):
        scaled = clip * low
        first_new = first_decay * first_old + (1.0 - first_decay) * scaled
        second_new = second_decay * second_old + (1.0 - second_decay) * scaled * scaled
        return first_new, second_new

    step = 2
    for k in range(0, CHIPS, step):
        low = low_all[k : k + step].reshape(16 * step, COLS)
        first_old = moments[2 * k : 2 * (k + step), 0].reshape(16 * step, COLS)
        second_old = moments[2 * k : 2 * (k + step), 1].reshape(16 * step, COLS)
        first_new, second_new = moved_by(low, first_old, second_old)
        ratio = first_new * lax.rsqrt(second_new)
        high = ratio.astype(bf16)
        ratios[0, 16 * k : 16 * (k + step)] = high
        ratios[1, 16 * k : 16 * (k + step)] = (ratio - high.astype(f32)).astype(bf16)
    left = factors[pl.ds(2 * own, 2)].reshape(256, RANK)
    added[...] = (
        jnp.dot(left, ratios[0], preferred_element_type=f32)
        + jnp.dot(left, ratios[1], preferred_element_type=f32)
    ).reshape(2, LANES, COLS)

    spread = Gather(2, 0, copies.at[c], pass_sem)
    for g in (0, 1):
        core = c if g == 0 else 1 - c
        for j in range(4):
            span = pl.ds(LANES * j, LANES)
            update = added[core, :, span]
            update = jnp.where(c == 0, update, update.T)
            fresh = weights[core, span] - learn_rate * update
            copies[c, 2 * own + core, span] = fresh.astype(bf16)
            if g == 0:
                new_weights[c, span] = fresh
            else:
                back[span] = fresh
        spread.start(g)
    for g in (0, 1):
        core = c if g == 0 else 1 - c
        first_new, second_new = moved_by(
            low_all[own, pl.ds(8 * core, 8)], moments[2 * own + core, 0], moments[2 * own + core, 1]
        )
        target = moved.at[c] if g == 0 else back_moved
        target[0] = first_new
        target[1] = second_new
    hand(5, back, new_weights.at[c])
    hand(6, back_moved, moved.at[c])
    gather.finish()
    moment_gather.finish()
    sent_off(factors.at[0], out_sem.at[0])
    sent_off(wide.at[0], out_sem.at[1])
    sent_off(moments.at[0], out_sem.at[2])
    sent_off(weights.at[0], out_sem.at[3])
    sent_off(right_in, out_sem.at[4])
    sent_off(cross_in, cross_sem.at[0])
    sent_off(cross_sq, sq_sem.at[0, 0])
    sent_off(last_sq, sq_sem.at[1, 0])
    sent_off(low_all.at[pl.ds(0, 3)], low_sem.at[0, 0])
    sent_off(low_all.at[pl.ds(0, 12)], low_sem.at[1, 0])
    for level in (1, 2, 3, 4):
        spread.take_level(level)
    sent_off(back, out_sem.at[5])
    sent_off(back_moved, out_sem.at[6])
    arrive(back, in_sem.at[5])
    arrive(back_moved, in_sem.at[6])
    for level in range(5):
        arrive(copies.at[0, pl.ds(0, 2 * len(LEVELS[level]))], pass_sem.at[level])
    spread.finish()


def write_kernel(new_weights, moved, copies, *rest):
    outs, sem = rest[:8], rest[8]
    new_v, first_v, second_v, copy_v, new_o, first_o, second_o, copy_o = outs
    pairs = []
    for j in range(4):
        span = pl.ds(LANES * j, LANES)
        pairs.append((copies.at[0, :, span], copy_v.at[:, :, span]))
        pairs.append((new_weights.at[0, span], new_v.at[:, span]))
    for k in range(2 * CHIPS):
        pairs.append((copies.at[1, k], copy_o.at[:, pl.ds(LANES * k, LANES)]))
    pairs += [
        (new_weights.at[1], new_o),
        (moved.at[0, 0], first_v),
        (moved.at[0, 1], second_v),
        (moved.at[1, 0], first_o),
        (moved.at[1, 1], second_o),
    ]
    started = [pltpu.make_async_copy(s, t, sem.at[k]) for k, (s, t) in enumerate(pairs)]
    for copy in started:
        copy.start()
    for copy in started:
        copy.wait()


def shards(*args):
    hbm = pl.BlockSpec(memory_space=pltpu.HBM)
    vmem = pl.BlockSpec(memory_space=pltpu.VMEM)
    dma = pltpu.SemaphoreType.DMA
    passed = pl.pallas_call(
        step_kernel,
        out_shape=(
            pltpu.VMEM((2, COLS, LANES), f32),
            pltpu.VMEM((2, 2, 8, COLS), f32),
            pltpu.VMEM((2, 2 * CHIPS, COLS, LANES), bf16),
        ),
        in_specs=[hbm] * 15,
        out_specs=(vmem,) * 3,
        scratch_shapes=[
            pltpu.VMEM((2, ROWS, COLS), bf16),
            pltpu.SMEM((HEADS_HERE,), f32),
            pltpu.VMEM((COLS,), f32),
            pltpu.VMEM((2, ROWS, WIDE), bf16),
            pltpu.VMEM((2, ROWS, COLS), bf16),
            pltpu.VMEM((ROWS, COLS), bf16),
            pltpu.VMEM((2 * CHIPS, LANES, RANK), bf16),
            pltpu.VMEM((2, COLS, LANES), f32),
            pltpu.VMEM((2 * CHIPS, 2, 8, COLS), f32),
            pltpu.VMEM((2, ROWS, RANK), f32),
            pltpu.VMEM((2, 2 * RANK, ROWS), bf16),
            pltpu.VMEM((CHIPS, 16, COLS), f32),
            pltpu.VMEM((CHIPS - 1, 16, COLS), f32),
            pltpu.VMEM((2, 8, LANES), f32),
            pltpu.VMEM((CHIPS - 1, 8, LANES), f32),
            pltpu.VMEM((7, 8, LANES), f32),
            pltpu.VMEM((CHIPS, 16, COLS), f32),
            pltpu.VMEM((2, RANK, COLS), bf16),
            pltpu.VMEM((2, LANES, COLS), f32),
            pltpu.VMEM((COLS, LANES), f32),
            pltpu.VMEM((2, 8, COLS), f32),
            dma((9,)),
            dma((7,)),
            dma((7,)),
            dma((3, 2)),
            dma((2, 2, 16)),
            dma((5,)),
            dma((2,)),
            dma((2, 2)),
            dma((2, 2)),
        ],
        compiler_params=pltpu.CompilerParams(
            collective_id=0, has_side_effects=True, vmem_limit_bytes=46 * 1024 * 1024
        ),
        name="step",
    )(*args)
    outs = pl.pallas_call(
        write_kernel,
        out_shape=(
            jax.ShapeDtypeStruct((LANES, COLS), f32),
            jax.ShapeDtypeStruct((8, COLS), f32),
            jax.ShapeDtypeStruct((8, COLS), f32),
            jax.ShapeDtypeStruct((2 * CHIPS, LANES, COLS), bf16),
            jax.ShapeDtypeStruct((COLS, LANES), f32),
            jax.ShapeDtypeStruct((8, COLS), f32),
            jax.ShapeDtypeStruct((8, COLS), f32),
            jax.ShapeDtypeStruct((COLS, WIDE), bf16),
        ),
        in_specs=[vmem] * 3,
        out_specs=(hbm,) * 8,
        scratch_shapes=[dma((2 * CHIPS + 13,))],
        compiler_params=pltpu.CompilerParams(vmem_limit_bytes=4 * 1024 * 1024),
        name="write",
    )(*passed)
    return (*outs[:3], outs[3].reshape(WIDE, COLS), *outs[4:])


def solution(mesh):
    torus = Mesh(mesh.devices.reshape(4, 4, 2, 4), ("z", "y", "c", "x"))
    split = P(FS, "x")
    whole = P(FS, None)
    return jax.shard_map(
        shards,
        mesh=torus,
        in_specs=(
            split, split, P("x"), P("x"), whole, whole, split, whole, whole,
            split, P("x", FS), split, split, split, split,
        ),
        out_specs=(
            split, split, split, P(None, "x"), P("x", FS), split, split, P("x", None),
        ),
        check_vma=False,
    )
```

```python
import math

import jax
import jax.numpy as jnp
from jax import lax
from jax.experimental import pallas as pl
from jax.experimental.pallas import tpu as pltpu
from jax.sharding import Mesh
from jax.sharding import PartitionSpec as P

MESH = pl.DeviceIdType.MESH
RANK = 256
HV = 2048
FS = ("z", "y", "c")

norm_epsilon = 1e-06
first_decay = 0.9
second_decay = 0.95
learn_rate = 0.1

ROWS = 768
WIDE = 4096
COLS = 512
HEADS_HERE = 4
CHIPS = 16
LANES = 128

f32 = jnp.float32
bf16 = jnp.bfloat16

LEVELS = (
    ((0, 0),),
    ((3, 0), (1, 0), (0, 3), (0, 1)),
    ((2, 0), (3, 3), (3, 1), (1, 3), (1, 1), (0, 2)),
    ((2, 3), (2, 1), (3, 2), (1, 2)),
    ((2, 2),),
)
GROUPS = (
    (),
    (((3, 0),), ((1, 0),), ((0, 3), (0, 1))),
    (((2, 0),), ((3, 3), (3, 1), (1, 3), (1, 1), (0, 2))),
    (((2, 3), (2, 1)), ((3, 2), (1, 2))),
    (((2, 2),),),
)
GROUP_OF = {p: k for k, group in enumerate(sum(GROUPS, ())) for p in group}


def step_kernel(
    first_map, second_map, lambda_head, head_gain, cot_output, layer_input, cot_values,
    factor_value, factor_output, weight_value, weight_output,
    first_value, second_value, first_output, second_output,
    new_weights, moved, copies,
    maps, lam, gain, wide, rights, right_in, factors, weights, moments,
    acc, turned, summed, cross_in, squares, cross_sq, last_sq, low_all, ratios, added, back, back_moved,
    load_sem, out_sem, in_sem, send_sem, recv_sem, moment_sem, pass_sem, cross_sem, sq_sem, low_sem,
):
    z, y, c, x = (lax.axis_index(a) for a in ("z", "y", "c", "x"))
    own = 4 * z + y
    mine = 2 * own + c
    partner = (z, y, 1 - c, x)

    def near(z_by, y_by, c_by, x_by):
        return (
            lax.rem(z + z_by, 4), lax.rem(y + y_by, 4), lax.rem(c + c_by, 2), lax.rem(x + x_by, 4)
        )

    def at(dz, dy):
        return 4 * lax.rem(z + dz, 4) + lax.rem(y + dy, 4)

    def place(da, db):
        return at(da * c + db * (1 - c), da * (1 - c) + db * c)

    def chip_at(da, db):
        return near(da * c + db * (1 - c), da * (1 - c) + db * c, 0, 0)

    def remote(source, target, sent, arrived, device):
        return pltpu.make_async_remote_copy(
            source, target, sent, arrived, device_id=device, device_id_type=MESH
        )

    def arrive(block, semaphore):
        remote(block, block, out_sem.at[0], semaphore, partner).wait_recv()

    def sent_off(block, semaphore):
        remote(block, block, semaphore, in_sem.at[0], partner).wait_send()

    def load(k, source, target):
        copy = pltpu.make_async_copy(source, target, load_sem.at[k])
        copy.start()

    def loaded(k, target):
        pltpu.make_async_copy(target, target, load_sem.at[k]).wait()

    value_args = (factor_value, first_value, second_value, layer_input)
    output_args = (factor_output, first_output, second_output, cot_output)

    def columns(ref, j):
        return ref.at[:, pl.ds(LANES * j, LANES)]

    def rows(ref, j):
        return ref.at[pl.ds(LANES * j, LANES)]

    def load_first(args):
        load(0, args[0], factors.at[mine])

    def load_later(args, weight, pieces):
        load(1, args[3], wide.at[0])
        load(2, args[1], moments.at[mine, 0])
        load(2, args[2], moments.at[mine, 1])
        for j in range(4):
            load(3, pieces(weight, j), rows(weights.at[c], j))

    pl.when(c == 0)(lambda: load_first(value_args))
    pl.when(c == 1)(lambda: load_first(output_args))
    barrier = pltpu.get_barrier_semaphore()
    greeted = [chip_at(1, 0), chip_at(3, 0), chip_at(0, 1), chip_at(0, 3), partner]
    greeted += [near(0, 0, dc, dx) for dx in (1, 2, 3) for dc in (0, 1)]
    for device in greeted:
        pl.semaphore_signal(barrier, inc=1, device_id=device, device_id_type=MESH)
    load(4, first_map, maps.at[0])
    load(4, second_map, maps.at[1])
    load(5, lambda_head, lam)
    load(6, head_gain, gain)
    pl.when(c == 0)(lambda: load_later(value_args, weight_value, columns))
    pl.when(c == 1)(lambda: load_later(output_args, weight_output, rows))
    load(7, cot_values, rights.at[0])
    pl.semaphore_wait(barrier, len(greeted))

    def hand(k, source, target):
        remote(source, target, out_sem.at[k], in_sem.at[k], partner).start()

    def hand_later(args, weight, pieces):
        hand(1, args[3], wide.at[1])
        hand(2, args[1], moments.at[mine, 0])
        hand(2, args[2], moments.at[mine, 1])
        for j in range(4):
            hand(3, pieces(weight, j), rows(weights.at[c], j))

    pl.when(c == 0)(lambda: hand(0, factor_output, factors.at[mine]))
    pl.when(c == 1)(lambda: hand(0, factor_value, factors.at[mine]))

    class Gather:
        def __init__(self, stage, arrived, blocks, parts, passed=None):
            self.blocks, self.passed, self.sent = blocks, passed, send_sem.at[stage]
            self.parts, self.size = parts, blocks.shape[1] // parts
            self.pieces = [(g, s) for g in (0, 1) for s in range(parts)]
            self.counts = [0, 0]
            self.arrived = arrived

        def piece(self, g, s, da, db):
            block = self.blocks.at[2 * place(da, db) + (c if g == 0 else 1 - c)]
            return block.at[pl.ds(self.size * s, self.size)]

        def fire(self, g, s, da, db, *ways):
            block = self.piece(g, s, da, db)
            for way in ways:
                ra, rb = da, db
                by = 1 if way[1] == "+" else 3
                if way[0] == "a":
                    device, ra = chip_at(by, 0), (da - by) % 4
                else:
                    device, rb = chip_at(0, by), (db - by) % 4
                arrived = self.arrived.at[self.parts * g + s, GROUP_OF[ra, rb]]
                remote(block, block, self.sent.at[g], arrived, device).start()
                self.counts[g] += 1
            if self.passed is not None:
                remote(block, block, self.sent.at[g], self.passed, partner).start()
                self.counts[g] += 1

        def start(self, g):
            for s in range(self.parts):
                self.fire(g, s, 0, 0, "b+", "b-", "a+", "a-")

        def take(self, g, s, group):
            whole = self.blocks.at[pl.ds(0, len(group)), pl.ds(0, self.size)]
            arrive(whole, self.arrived.at[self.parts * g + s, GROUP_OF[group[0]]])
            even = (g + s) % 2 == 0
            for da, db in group:
                ways = []
                if db == 0:
                    if da == (3 if even else 1):
                        ways.append("a+" if even else "a-")
                    ways += ["b+", "b-"]
                elif db == (3 if (da in (0, 1)) == even else 1):
                    ways.append("b+" if db == 3 else "b-")
                self.fire(g, s, da, db, *ways)

        def take_level(self, level, only=None):
            for g, s in self.pieces:
                if only in (None, g):
                    for group in GROUPS[level]:
                        self.take(g, s, group)

        def finish(self):
            for g in (0, 1):
                sent_off(self.blocks.at[pl.ds(0, self.counts[g] // self.parts)], self.sent.at[g])

    loaded(0, factors.at[mine])
    gather = Gather(0, recv_sem, factors, 2)
    gather.start(0)
    pl.when(c == 0)(lambda: hand_later(output_args, weight_output, rows))
    pl.when(c == 1)(lambda: hand_later(value_args, weight_value, columns))
    loaded(4, maps)
    loaded(5, lam)
    loaded(6, gain)
    width = COLS // HEADS_HERE
    for h in range(HEADS_HERE):
        span = pl.ds(h * width, width)
        differ = maps[0, :, span].astype(f32) - lam[h] * maps[1, :, span].astype(f32)
        mean = jnp.sum(differ * differ, axis=-1, keepdims=True) * (1.0 / width)
        scaled = differ * lax.rsqrt(mean + norm_epsilon)
        rights[1, :, span] = (scaled * gain[span][None, :]).astype(bf16)
    arrive(factors.at[mine], in_sem.at[0])
    gather.start(1)
    loaded(7, rights.at[0])
    hand(4, rights.at[1 - c], right_in)

    def project(t, *chips, fresh=False):
        left = [wide[t, :, pl.ds(pl.multiple_of(p * 256, 256), 256)] for p in chips]
        right = [factors[pl.ds(2 * p, 2)].reshape(256, RANK) for p in chips]
        if len(chips) > 1:
            left, right = [jnp.concatenate(left, axis=1)], [jnp.concatenate(right, axis=0)]
        part = jnp.dot(left[0], right[0], preferred_element_type=f32)
        acc[t] = part if fresh else acc[t] + part

    PAIRS = (
        None,
        (((1, 0), (3, 0)), ((0, 1), (0, 3))),
        (((2, 0), (0, 2)), ((1, 1), (3, 3)), ((1, 3), (3, 1))),
        (((2, 1), (2, 3)), ((1, 2), (3, 2))),
    )

    def project_pairs(t, level, *which):
        for k in which:
            (z0, y0), (z1, y1) = PAIRS[level][k]
            project(t, at(z0, y0), at(z1, y1))

    gather.take_level(1)
    loaded(1, wide.at[0])
    project(0, own, fresh=True)
    gather.take_level(2, 0)
    project_pairs(0, 1, 0)
    gather.take_level(2, 1)
    project_pairs(0, 1, 1)
    gather.take_level(3, 0)
    arrive(wide.at[1], in_sem.at[1])
    project(1, own, fresh=True)
    project_pairs(1, 1, 0, 1)
    gather.take_level(3, 1)
    loaded(2, moments.at[mine])
    arrive(moments.at[mine], in_sem.at[2])
    moment_gather = Gather(1, moment_sem, moments, 1)
    moment_gather.start(0)
    moment_gather.start(1)
    project_pairs(0, 2, 0, 1, 2)
    project_pairs(1, 2, 0, 1)
    gather.take_level(4)
    project_pairs(1, 2, 2)
    for t in (0, 1):
        project_pairs(t, 3, 0, 1)
    moment_gather.take_level(1)
    for t in (0, 1):
        project(t, at(2, 2))

    arrive(right_in, in_sem.at[4])
    product = None
    for t in (0, 1):
        flat = acc[t].T
        high = flat.astype(bf16)
        turned[t, :RANK] = high
        turned[t, RANK:] = (flat - high.astype(f32)).astype(bf16)
        right = rights[c] if t == 0 else right_in[...]
        part = jnp.dot(turned[t], right, preferred_element_type=f32)
        product = part if t == 0 else product + part
    summed[...] = (product[:RANK] + product[RANK:]).reshape(CHIPS, 16, COLS)

    offsets = sorted(
        ((dz, dy) for dz in range(4) for dy in range(4) if (dz, dy) != (0, 0)),
        key=lambda o: -(min(o[0], 4 - o[0]) + min(o[1], 4 - o[1])),
    )
    for k, (dz, dy) in enumerate(offsets):
        remote(
            summed.at[at(dz, dy)], cross_in.at[k], cross_sem.at[0], cross_sem.at[1],
            near(dz, dy, 0, 0),
        ).start()
    arrive(cross_in, cross_sem.at[1])
    total = summed[own]
    for k in range(len(offsets)):
        total = total + cross_in[k]
    low_all[own] = total

    def fold(value):
        value = value[:8] + value[8:]
        return sum(value[:, LANES * j : LANES * (j + 1)] for j in range(COLS // LANES))

    squares[0] = fold(total * total)
    for k, (dz, dy) in enumerate(offsets):
        remote(
            squares.at[0], cross_sq.at[k], sq_sem.at[0, 0], sq_sem.at[0, 1], near(dz, dy, 0, 0)
        ).start()
    def send_low(block, way):
        for by in (2, 1, 3):
            device = chip_at(by, 0) if way == 0 else chip_at(0, by)
            remote(block, block, low_sem.at[way, 0], low_sem.at[way, 1], device).start()

    send_low(low_all.at[own], 0)
    send_low(low_all.at[own], 1)
    moment_gather.take_level(2)
    arrive(low_all.at[pl.ds(0, 3)], low_sem.at[0, 1])
    for k in (2, 1, 3):
        send_low(low_all.at[place(k, 0)], 1)
    arrive(cross_sq, sq_sem.at[0, 1])
    plane = squares[0]
    for k in range(len(offsets)):
        plane = plane + cross_sq[k]
    squares[1] = plane
    for k, (dx, dc) in enumerate(((2, 1), (1, 1), (3, 1), (2, 0), (1, 0), (3, 0), (0, 1))):
        remote(
            squares.at[1], last_sq.at[k], sq_sem.at[1, 0], sq_sem.at[1, 1], near(0, 0, dc, dx)
        ).start()
    moment_gather.take_level(3)
    arrive(weights.at[0], in_sem.at[3])
    loaded(3, weights.at[0])
    arrive(low_all.at[pl.ds(0, 12)], low_sem.at[1, 1])
    arrive(last_sq, sq_sem.at[1, 1])
    whole = squares[1]
    for k in range(7):
        whole = whole + last_sq[k]
    square_sum = jnp.sum(jnp.sum(whole, axis=1, keepdims=True), axis=0, keepdims=True)
    clip = jnp.minimum(1.0, math.sqrt(RANK * HV) * lax.rsqrt(square_sum + norm_epsilon))

    moment_gather.take_level(4)
    def moved_by(low, first_old, second_old):
        scaled = clip * low
        first_new = first_decay * first_old + (1.0 - first_decay) * scaled
        second_new = second_decay * second_old + (1.0 - second_decay) * scaled * scaled
        return first_new, second_new

    step = 2
    for k in range(0, CHIPS, step):
        low = low_all[k : k + step].reshape(16 * step, COLS)
        first_old = moments[2 * k : 2 * (k + step), 0].reshape(16 * step, COLS)
        second_old = moments[2 * k : 2 * (k + step), 1].reshape(16 * step, COLS)
        first_new, second_new = moved_by(low, first_old, second_old)
        ratio = first_new * lax.rsqrt(second_new)
        high = ratio.astype(bf16)
        ratios[0, 16 * k : 16 * (k + step)] = high
        ratios[1, 16 * k : 16 * (k + step)] = (ratio - high.astype(f32)).astype(bf16)
    left = factors[pl.ds(2 * own, 2)].reshape(256, RANK)
    added[...] = (
        jnp.dot(left, ratios[0], preferred_element_type=f32)
        + jnp.dot(left, ratios[1], preferred_element_type=f32)
    ).reshape(2, LANES, COLS)

    spread = Gather(2, recv_sem, copies.at[c], 2, passed=pass_sem.at[0])
    for g in (0, 1):
        core = c if g == 0 else 1 - c
        for j in range(4):
            span = pl.ds(LANES * j, LANES)
            update = added[core, :, span]
            update = jnp.where(c == 0, update, update.T)
            fresh = weights[core, span] - learn_rate * update
            copies[c, 2 * own + core, span] = fresh.astype(bf16)
            if g == 0:
                new_weights[c, span] = fresh
            else:
                back[span] = fresh
        spread.start(g)
    for g in (0, 1):
        core = c if g == 0 else 1 - c
        first_new, second_new = moved_by(
            low_all[own, pl.ds(8 * core, 8)], moments[2 * own + core, 0], moments[2 * own + core, 1]
        )
        target = moved.at[c] if g == 0 else back_moved
        target[0] = first_new
        target[1] = second_new
    hand(5, back, new_weights.at[c])
    hand(6, back_moved, moved.at[c])
    gather.finish()
    moment_gather.finish()
    sent_off(factors.at[0], out_sem.at[0])
    sent_off(wide.at[0], out_sem.at[1])
    sent_off(moments.at[0], out_sem.at[2])
    sent_off(weights.at[0], out_sem.at[3])
    sent_off(right_in, out_sem.at[4])
    sent_off(cross_in, cross_sem.at[0])
    sent_off(cross_sq, sq_sem.at[0, 0])
    sent_off(last_sq, sq_sem.at[1, 0])
    sent_off(low_all.at[pl.ds(0, 3)], low_sem.at[0, 0])
    sent_off(low_all.at[pl.ds(0, 12)], low_sem.at[1, 0])
    for level in (1, 2, 3, 4):
        spread.take_level(level)
    sent_off(back, out_sem.at[5])
    sent_off(back_moved, out_sem.at[6])
    arrive(back, in_sem.at[5])
    arrive(back_moved, in_sem.at[6])
    arrive(copies.at[0], pass_sem.at[0])
    spread.finish()


def write_kernel(new_weights, moved, copies, *rest):
    outs, sem = rest[:8], rest[8]
    new_v, first_v, second_v, copy_v, new_o, first_o, second_o, copy_o = outs
    for j in range(4):
        span = pl.ds(LANES * j, LANES)
        pltpu.make_async_copy(copies.at[0, :, span], copy_v.at[:, :, span], sem.at[0]).start()
        pltpu.make_async_copy(new_weights.at[0, span], new_v.at[:, span], sem.at[1]).start()
    for k in range(2 * CHIPS):
        target = copy_o.at[:, pl.ds(LANES * k, LANES)]
        pltpu.make_async_copy(copies.at[1, k], target, sem.at[0]).start()
    pltpu.make_async_copy(new_weights.at[1], new_o, sem.at[1]).start()
    for k, target in enumerate((first_v, second_v, first_o, second_o)):
        pltpu.make_async_copy(moved.at[k // 2, k % 2], target, sem.at[2]).start()
    for k, source in enumerate((copies, new_weights, moved)):
        pltpu.make_async_copy(source, source, sem.at[k]).wait()


def shards(*args):
    hbm = pl.BlockSpec(memory_space=pltpu.HBM)
    vmem = pl.BlockSpec(memory_space=pltpu.VMEM)
    dma = pltpu.SemaphoreType.DMA
    passed = pl.pallas_call(
        step_kernel,
        out_shape=(
            pltpu.VMEM((2, COLS, LANES), f32),
            pltpu.VMEM((2, 2, 8, COLS), f32),
            pltpu.VMEM((2, 2 * CHIPS, COLS, LANES), bf16),
        ),
        in_specs=[hbm] * 15,
        out_specs=(vmem,) * 3,
        scratch_shapes=[
            pltpu.VMEM((2, ROWS, COLS), bf16),
            pltpu.SMEM((HEADS_HERE,), f32),
            pltpu.VMEM((COLS,), f32),
            pltpu.VMEM((2, ROWS, WIDE), bf16),
            pltpu.VMEM((2, ROWS, COLS), bf16),
            pltpu.VMEM((ROWS, COLS), bf16),
            pltpu.VMEM((2 * CHIPS, LANES, RANK), bf16),
            pltpu.VMEM((2, COLS, LANES), f32),
            pltpu.VMEM((2 * CHIPS, 2, 8, COLS), f32),
            pltpu.VMEM((2, ROWS, RANK), f32),
            pltpu.VMEM((2, 2 * RANK, ROWS), bf16),
            pltpu.VMEM((CHIPS, 16, COLS), f32),
            pltpu.VMEM((CHIPS - 1, 16, COLS), f32),
            pltpu.VMEM((2, 8, LANES), f32),
            pltpu.VMEM((CHIPS - 1, 8, LANES), f32),
            pltpu.VMEM((7, 8, LANES), f32),
            pltpu.VMEM((CHIPS, 16, COLS), f32),
            pltpu.VMEM((2, RANK, COLS), bf16),
            pltpu.VMEM((2, LANES, COLS), f32),
            pltpu.VMEM((COLS, LANES), f32),
            pltpu.VMEM((2, 8, COLS), f32),
            dma((8,)),
            dma((7,)),
            dma((7,)),
            dma((3, 2)),
            dma((4, 8)),
            dma((2, 8)),
            dma((1,)),
            dma((2,)),
            dma((2, 2)),
            dma((2, 2)),
        ],
        compiler_params=pltpu.CompilerParams(
            collective_id=0, has_side_effects=True, vmem_limit_bytes=46 * 1024 * 1024
        ),
        name="step",
    )(*args)
    outs = pl.pallas_call(
        write_kernel,
        out_shape=(
            jax.ShapeDtypeStruct((LANES, COLS), f32),
            jax.ShapeDtypeStruct((8, COLS), f32),
            jax.ShapeDtypeStruct((8, COLS), f32),
            jax.ShapeDtypeStruct((2 * CHIPS, LANES, COLS), bf16),
            jax.ShapeDtypeStruct((COLS, LANES), f32),
            jax.ShapeDtypeStruct((8, COLS), f32),
            jax.ShapeDtypeStruct((8, COLS), f32),
            jax.ShapeDtypeStruct((COLS, WIDE), bf16),
        ),
        in_specs=[vmem] * 3,
        out_specs=(hbm,) * 8,
        scratch_shapes=[dma((3,))],
        compiler_params=pltpu.CompilerParams(vmem_limit_bytes=4 * 1024 * 1024),
        name="write",
    )(*passed)
    return (*outs[:3], outs[3].reshape(WIDE, COLS), *outs[4:])


def solution(mesh):
    torus = Mesh(mesh.devices.reshape(4, 4, 2, 4), ("z", "y", "c", "x"))
    split = P(FS, "x")
    whole = P(FS, None)
    return jax.shard_map(
        shards,
        mesh=torus,
        in_specs=(
            split, split, P("x"), P("x"), whole, whole, split, whole, whole,
            split, P("x", FS), split, split, split, split,
        ),
        out_specs=(
            split, split, split, P(None, "x"), P("x", FS), split, split, P("x", None),
        ),
        check_vma=False,
    )
```

```python
import math

import jax
import jax.numpy as jnp
from jax import lax
from jax.experimental import pallas as pl
from jax.experimental.pallas import tpu as pltpu
from jax.sharding import Mesh
from jax.sharding import PartitionSpec as P

MESH = pl.DeviceIdType.MESH
RANK = 256
HV = 2048
FS = ("z", "y", "c")

norm_epsilon = 1e-06
first_decay = 0.9
second_decay = 0.95
learn_rate = 0.1

ROWS = 768
WIDE = 4096
COLS = 512
HEADS_HERE = 4
CHIPS = 16
LANES = 128

f32 = jnp.float32
bf16 = jnp.bfloat16

LEVELS = (
    ((0, 0),),
    ((3, 0), (1, 0), (0, 3), (0, 1)),
    ((2, 0), (3, 3), (3, 1), (1, 3), (1, 1), (0, 2)),
    ((2, 3), (2, 1), (3, 2), (1, 2)),
    ((2, 2),),
)
GROUPS = (
    (),
    (((3, 0),), ((1, 0),), ((0, 3), (0, 1))),
    (((2, 0),), ((3, 3), (3, 1), (1, 3), (1, 1), (0, 2))),
    (((2, 3), (2, 1)), ((3, 2), (1, 2))),
    (((2, 2),),),
)
GROUP_OF = {p: k for k, group in enumerate(sum(GROUPS, ())) for p in group}


def step_kernel(
    first_map, second_map, lambda_head, head_gain, cot_output, layer_input, cot_values,
    factor_value, factor_output, weight_value, weight_output,
    first_value, second_value, first_output, second_output,
    new_weights, moved, copies,
    maps, lam, gain, wide, rights, right_in, factors, other_rows, weights, moments,
    acc, turned, summed, cross_in, squares, cross_sq, last_sq, low_all, ratios, added, back, back_moved,
    load_sem, out_sem, in_sem, send_sem, recv_sem, moment_sem, pass_sem, cross_sem, sq_sem, low_sem,
):
    z, y, c, x = (lax.axis_index(a) for a in ("z", "y", "c", "x"))
    own = 4 * z + y
    mine = 2 * own + c
    partner = (z, y, 1 - c, x)

    def near(z_by, y_by, c_by, x_by):
        return (
            lax.rem(z + z_by, 4), lax.rem(y + y_by, 4), lax.rem(c + c_by, 2), lax.rem(x + x_by, 4)
        )

    def at(dz, dy):
        return 4 * lax.rem(z + dz, 4) + lax.rem(y + dy, 4)

    def place(da, db):
        return at(da * c + db * (1 - c), da * (1 - c) + db * c)

    def chip_at(da, db):
        return near(da * c + db * (1 - c), da * (1 - c) + db * c, 0, 0)

    def remote(source, target, sent, arrived, device):
        return pltpu.make_async_remote_copy(
            source, target, sent, arrived, device_id=device, device_id_type=MESH
        )

    def arrive(block, semaphore):
        remote(block, block, out_sem.at[0], semaphore, partner).wait_recv()

    def sent_off(block, semaphore):
        remote(block, block, semaphore, in_sem.at[0], partner).wait_send()

    def load(k, source, target):
        copy = pltpu.make_async_copy(source, target, load_sem.at[k])
        copy.start()

    def loaded(k, target):
        pltpu.make_async_copy(target, target, load_sem.at[k]).wait()

    value_args = (first_value, second_value, layer_input)
    output_args = (first_output, second_output, cot_output)

    def columns(ref, j):
        return ref.at[:, pl.ds(LANES * j, LANES)]

    def rows(ref, j):
        return ref.at[pl.ds(LANES * j, LANES)]

    def load_first(own_factor, other_factor):
        load(0, own_factor, factors.at[mine])
        load(8, other_factor, other_rows)

    def load_later(args, weight, pieces):
        load(1, args[2], wide.at[0])
        load(2, args[0], moments.at[mine, 0])
        load(2, args[1], moments.at[mine, 1])
        for j in range(4):
            load(3, pieces(weight, j), rows(weights.at[c], j))

    pl.when(c == 0)(lambda: load_first(factor_value, factor_output))
    pl.when(c == 1)(lambda: load_first(factor_output, factor_value))
    barrier = pltpu.get_barrier_semaphore()
    greeted = [chip_at(1, 0), chip_at(3, 0), chip_at(0, 1), chip_at(0, 3), partner]
    greeted += [near(0, 0, dc, dx) for dx in (1, 2, 3) for dc in (0, 1)]
    for device in greeted:
        pl.semaphore_signal(barrier, inc=1, device_id=device, device_id_type=MESH)
    load(4, first_map, maps.at[0])
    load(4, second_map, maps.at[1])
    load(5, lambda_head, lam)
    load(6, head_gain, gain)
    pl.when(c == 0)(lambda: load_later(value_args, weight_value, columns))
    pl.when(c == 1)(lambda: load_later(output_args, weight_output, rows))
    load(7, cot_values, rights.at[0])
    pl.semaphore_wait(barrier, len(greeted))

    def hand(k, source, target):
        remote(source, target, out_sem.at[k], in_sem.at[k], partner).start()

    def hand_later(args, weight, pieces):
        hand(1, args[2], wide.at[1])
        hand(2, args[0], moments.at[mine, 0])
        hand(2, args[1], moments.at[mine, 1])
        for j in range(4):
            hand(3, pieces(weight, j), rows(weights.at[c], j))

    loaded(8, other_rows)
    hand(0, other_rows, factors.at[mine])

    class Gather:
        def __init__(self, stage, arrived, blocks, parts, passed=None):
            self.blocks, self.passed, self.sent = blocks, passed, send_sem.at[stage]
            self.parts, self.size = parts, blocks.shape[1] // parts
            self.pieces = [(g, s) for g in (0, 1) for s in range(parts)]
            self.counts = [0, 0]
            self.arrived = arrived

        def piece(self, g, s, da, db):
            block = self.blocks.at[2 * place(da, db) + (c if g == 0 else 1 - c)]
            return block.at[pl.ds(self.size * s, self.size)]

        def fire(self, g, s, da, db, *ways):
            block = self.piece(g, s, da, db)
            for way in ways:
                ra, rb = da, db
                by = 1 if way[1] == "+" else 3
                if way[0] == "a":
                    device, ra = chip_at(by, 0), (da - by) % 4
                else:
                    device, rb = chip_at(0, by), (db - by) % 4
                arrived = self.arrived.at[self.parts * g + s, GROUP_OF[ra, rb]]
                remote(block, block, self.sent.at[g], arrived, device).start()
                self.counts[g] += 1
            if self.passed is not None:
                remote(block, block, self.sent.at[g], self.passed, partner).start()
                self.counts[g] += 1

        def start(self, g):
            for s in range(self.parts):
                self.fire(g, s, 0, 0, "b+", "b-", "a+", "a-")

        def take(self, g, s, group):
            whole = self.blocks.at[pl.ds(0, len(group)), pl.ds(0, self.size)]
            arrive(whole, self.arrived.at[self.parts * g + s, GROUP_OF[group[0]]])
            even = (g + s) % 2 == 0
            for da, db in group:
                ways = []
                if db == 0:
                    if da == (3 if even else 1):
                        ways.append("a+" if even else "a-")
                    ways += ["b+", "b-"]
                elif db == (3 if (da in (0, 1)) == even else 1):
                    ways.append("b+" if db == 3 else "b-")
                self.fire(g, s, da, db, *ways)

        def take_level(self, level, only=None):
            for g, s in self.pieces:
                if only in (None, g):
                    for group in GROUPS[level]:
                        self.take(g, s, group)

        def finish(self):
            for g in (0, 1):
                sent_off(self.blocks.at[pl.ds(0, self.counts[g] // self.parts)], self.sent.at[g])

    loaded(0, factors.at[mine])
    gather = Gather(0, recv_sem, factors, 2)
    gather.start(0)
    pl.when(c == 0)(lambda: hand_later(output_args, weight_output, rows))
    pl.when(c == 1)(lambda: hand_later(value_args, weight_value, columns))
    loaded(4, maps)
    loaded(5, lam)
    loaded(6, gain)
    width = COLS // HEADS_HERE
    for h in range(HEADS_HERE):
        span = pl.ds(h * width, width)
        differ = maps[0, :, span].astype(f32) - lam[h] * maps[1, :, span].astype(f32)
        mean = jnp.sum(differ * differ, axis=-1, keepdims=True) * (1.0 / width)
        scaled = differ * lax.rsqrt(mean + norm_epsilon)
        rights[1, :, span] = (scaled * gain[span][None, :]).astype(bf16)
    arrive(factors.at[mine], in_sem.at[0])
    gather.start(1)
    loaded(7, rights.at[0])
    hand(4, rights.at[1 - c], right_in)

    def project(t, *chips, fresh=False):
        left = [wide[t, :, pl.ds(pl.multiple_of(p * 256, 256), 256)] for p in chips]
        right = [factors[pl.ds(2 * p, 2)].reshape(256, RANK) for p in chips]
        if len(chips) > 1:
            left, right = [jnp.concatenate(left, axis=1)], [jnp.concatenate(right, axis=0)]
        part = jnp.dot(left[0], right[0], preferred_element_type=f32)
        acc[t] = part if fresh else acc[t] + part

    PAIRS = (
        None,
        (((1, 0), (3, 0)), ((0, 1), (0, 3))),
        (((2, 0), (0, 2)), ((1, 1), (3, 3)), ((1, 3), (3, 1))),
        (((2, 1), (2, 3)), ((1, 2), (3, 2))),
    )

    def project_pairs(t, level, *which):
        for k in which:
            (z0, y0), (z1, y1) = PAIRS[level][k]
            project(t, at(z0, y0), at(z1, y1))

    gather.take_level(1)
    loaded(1, wide.at[0])
    project(0, own, fresh=True)
    gather.take_level(2, 0)
    project_pairs(0, 1, 0)
    gather.take_level(2, 1)
    project_pairs(0, 1, 1)
    gather.take_level(3, 0)
    arrive(wide.at[1], in_sem.at[1])
    project(1, own, fresh=True)
    project_pairs(1, 1, 0, 1)
    gather.take_level(3, 1)
    loaded(2, moments.at[mine])
    arrive(moments.at[mine], in_sem.at[2])
    moment_gather = Gather(1, moment_sem, moments, 1)
    moment_gather.start(0)
    moment_gather.start(1)
    project_pairs(0, 2, 0, 1, 2)
    project_pairs(1, 2, 0, 1, 2)
    for t in (0, 1):
        project_pairs(t, 3, 0, 1)
    gather.take_level(4)
    for t in (0, 1):
        project(t, at(2, 2))

    arrive(right_in, in_sem.at[4])
    product = None
    for t in (0, 1):
        flat = acc[t].T
        high = flat.astype(bf16)
        turned[t, :RANK] = high
        turned[t, RANK:] = (flat - high.astype(f32)).astype(bf16)
        right = rights[c] if t == 0 else right_in[...]
        part = jnp.dot(turned[t], right, preferred_element_type=f32)
        product = part if t == 0 else product + part
    summed[...] = (product[:RANK] + product[RANK:]).reshape(CHIPS, 16, COLS)

    offsets = sorted(
        ((dz, dy) for dz in range(4) for dy in range(4) if (dz, dy) != (0, 0)),
        key=lambda o: -(min(o[0], 4 - o[0]) + min(o[1], 4 - o[1])),
    )
    for k, (dz, dy) in enumerate(offsets):
        remote(
            summed.at[at(dz, dy)], cross_in.at[k], cross_sem.at[0], cross_sem.at[1],
            near(dz, dy, 0, 0),
        ).start()
    moment_gather.take_level(1)
    arrive(cross_in, cross_sem.at[1])
    total = summed[own]
    for k in range(len(offsets)):
        total = total + cross_in[k]
    low_all[own] = total

    def fold(value):
        value = value[:8] + value[8:]
        return sum(value[:, LANES * j : LANES * (j + 1)] for j in range(COLS // LANES))

    squares[0] = fold(total * total)
    for k, (dz, dy) in enumerate(offsets):
        remote(
            squares.at[0], cross_sq.at[k], sq_sem.at[0, 0], sq_sem.at[0, 1], near(dz, dy, 0, 0)
        ).start()
    def send_low(block, way):
        for by in (2, 1, 3):
            device = chip_at(by, 0) if way == 0 else chip_at(0, by)
            remote(block, block, low_sem.at[way, 0], low_sem.at[way, 1], device).start()

    send_low(low_all.at[own], 0)
    send_low(low_all.at[own], 1)
    moment_gather.take_level(2)
    arrive(cross_sq, sq_sem.at[0, 1])
    plane = squares[0]
    for k in range(len(offsets)):
        plane = plane + cross_sq[k]
    squares[1] = plane
    for k, (dx, dc) in enumerate(((2, 1), (1, 1), (3, 1), (2, 0), (1, 0), (3, 0), (0, 1))):
        remote(
            squares.at[1], last_sq.at[k], sq_sem.at[1, 0], sq_sem.at[1, 1], near(0, 0, dc, dx)
        ).start()
    arrive(low_all.at[pl.ds(0, 3)], low_sem.at[0, 1])
    for k in (2, 1, 3):
        send_low(low_all.at[place(k, 0)], 1)
    moment_gather.take_level(3)
    arrive(weights.at[0], in_sem.at[3])
    loaded(3, weights.at[0])
    arrive(low_all.at[pl.ds(0, 12)], low_sem.at[1, 1])
    arrive(last_sq, sq_sem.at[1, 1])
    whole = squares[1]
    for k in range(7):
        whole = whole + last_sq[k]
    square_sum = jnp.sum(jnp.sum(whole, axis=1, keepdims=True), axis=0, keepdims=True)
    clip = jnp.minimum(1.0, math.sqrt(RANK * HV) * lax.rsqrt(square_sum + norm_epsilon))

    moment_gather.take_level(4)
    def moved_by(low, first_old, second_old):
        scaled = clip * low
        first_new = first_decay * first_old + (1.0 - first_decay) * scaled
        second_new = second_decay * second_old + (1.0 - second_decay) * scaled * scaled
        return first_new, second_new

    step = 2
    for k in range(0, CHIPS, step):
        low = low_all[k : k + step].reshape(16 * step, COLS)
        first_old = moments[2 * k : 2 * (k + step), 0].reshape(16 * step, COLS)
        second_old = moments[2 * k : 2 * (k + step), 1].reshape(16 * step, COLS)
        first_new, second_new = moved_by(low, first_old, second_old)
        ratio = first_new * lax.rsqrt(second_new)
        high = ratio.astype(bf16)
        ratios[0, 16 * k : 16 * (k + step)] = high
        ratios[1, 16 * k : 16 * (k + step)] = (ratio - high.astype(f32)).astype(bf16)
    left = factors[pl.ds(2 * own, 2)].reshape(256, RANK)
    added[...] = (
        jnp.dot(left, ratios[0], preferred_element_type=f32)
        + jnp.dot(left, ratios[1], preferred_element_type=f32)
    ).reshape(2, LANES, COLS)

    spread = Gather(2, recv_sem, copies.at[c], 2, passed=pass_sem.at[0])
    for g in (0, 1):
        core = c if g == 0 else 1 - c
        for j in range(4):
            span = pl.ds(LANES * j, LANES)
            update = added[core, :, span]
            update = jnp.where(c == 0, update, update.T)
            fresh = weights[core, span] - learn_rate * update
            copies[c, 2 * own + core, span] = fresh.astype(bf16)
            if g == 0:
                new_weights[c, span] = fresh
            else:
                back[span] = fresh
        spread.start(g)
    for g in (0, 1):
        core = c if g == 0 else 1 - c
        first_new, second_new = moved_by(
            low_all[own, pl.ds(8 * core, 8)], moments[2 * own + core, 0], moments[2 * own + core, 1]
        )
        target = moved.at[c] if g == 0 else back_moved
        target[0] = first_new
        target[1] = second_new
    hand(5, back, new_weights.at[c])
    hand(6, back_moved, moved.at[c])
    gather.finish()
    moment_gather.finish()
    sent_off(factors.at[0], out_sem.at[0])
    sent_off(wide.at[0], out_sem.at[1])
    sent_off(moments.at[0], out_sem.at[2])
    sent_off(weights.at[0], out_sem.at[3])
    sent_off(right_in, out_sem.at[4])
    sent_off(cross_in, cross_sem.at[0])
    sent_off(cross_sq, sq_sem.at[0, 0])
    sent_off(last_sq, sq_sem.at[1, 0])
    sent_off(low_all.at[pl.ds(0, 3)], low_sem.at[0, 0])
    sent_off(low_all.at[pl.ds(0, 12)], low_sem.at[1, 0])
    for level in (1, 2, 3, 4):
        spread.take_level(level)
    sent_off(back, out_sem.at[5])
    sent_off(back_moved, out_sem.at[6])
    arrive(back, in_sem.at[5])
    arrive(back_moved, in_sem.at[6])
    arrive(copies.at[0], pass_sem.at[0])
    spread.finish()


def write_kernel(new_weights, moved, copies, *rest):
    outs, sem = rest[:8], rest[8]
    new_v, first_v, second_v, copy_v, new_o, first_o, second_o, copy_o = outs
    for j in range(4):
        span = pl.ds(LANES * j, LANES)
        pltpu.make_async_copy(copies.at[0, :, span], copy_v.at[:, :, span], sem.at[0]).start()
        pltpu.make_async_copy(new_weights.at[0, span], new_v.at[:, span], sem.at[1]).start()
    for k in range(2 * CHIPS):
        target = copy_o.at[:, pl.ds(LANES * k, LANES)]
        pltpu.make_async_copy(copies.at[1, k], target, sem.at[0]).start()
    pltpu.make_async_copy(new_weights.at[1], new_o, sem.at[1]).start()
    for k, target in enumerate((first_v, second_v, first_o, second_o)):
        pltpu.make_async_copy(moved.at[k // 2, k % 2], target, sem.at[2]).start()
    for k, source in enumerate((copies, new_weights, moved)):
        pltpu.make_async_copy(source, source, sem.at[k]).wait()


def shards(*args):
    hbm = pl.BlockSpec(memory_space=pltpu.HBM)
    vmem = pl.BlockSpec(memory_space=pltpu.VMEM)
    dma = pltpu.SemaphoreType.DMA
    passed = pl.pallas_call(
        step_kernel,
        out_shape=(
            pltpu.VMEM((2, COLS, LANES), f32),
            pltpu.VMEM((2, 2, 8, COLS), f32),
            pltpu.VMEM((2, 2 * CHIPS, COLS, LANES), bf16),
        ),
        in_specs=[hbm] * 15,
        out_specs=(vmem,) * 3,
        scratch_shapes=[
            pltpu.VMEM((2, ROWS, COLS), bf16),
            pltpu.SMEM((HEADS_HERE,), f32),
            pltpu.VMEM((COLS,), f32),
            pltpu.VMEM((2, ROWS, WIDE), bf16),
            pltpu.VMEM((2, ROWS, COLS), bf16),
            pltpu.VMEM((ROWS, COLS), bf16),
            pltpu.VMEM((2 * CHIPS, LANES, RANK), bf16),
            pltpu.VMEM((LANES, RANK), bf16),
            pltpu.VMEM((2, COLS, LANES), f32),
            pltpu.VMEM((2 * CHIPS, 2, 8, COLS), f32),
            pltpu.VMEM((2, ROWS, RANK), f32),
            pltpu.VMEM((2, 2 * RANK, ROWS), bf16),
            pltpu.VMEM((CHIPS, 16, COLS), f32),
            pltpu.VMEM((CHIPS - 1, 16, COLS), f32),
            pltpu.VMEM((2, 8, LANES), f32),
            pltpu.VMEM((CHIPS - 1, 8, LANES), f32),
            pltpu.VMEM((7, 8, LANES), f32),
            pltpu.VMEM((CHIPS, 16, COLS), f32),
            pltpu.VMEM((2, RANK, COLS), bf16),
            pltpu.VMEM((2, LANES, COLS), f32),
            pltpu.VMEM((COLS, LANES), f32),
            pltpu.VMEM((2, 8, COLS), f32),
            dma((9,)),
            dma((7,)),
            dma((7,)),
            dma((3, 2)),
            dma((4, 8)),
            dma((2, 8)),
            dma((1,)),
            dma((2,)),
            dma((2, 2)),
            dma((2, 2)),
        ],
        compiler_params=pltpu.CompilerParams(
            collective_id=0, has_side_effects=True, vmem_limit_bytes=46 * 1024 * 1024
        ),
        name="step",
    )(*args)
    outs = pl.pallas_call(
        write_kernel,
        out_shape=(
            jax.ShapeDtypeStruct((LANES, COLS), f32),
            jax.ShapeDtypeStruct((8, COLS), f32),
            jax.ShapeDtypeStruct((8, COLS), f32),
            jax.ShapeDtypeStruct((2 * CHIPS, LANES, COLS), bf16),
            jax.ShapeDtypeStruct((COLS, LANES), f32),
            jax.ShapeDtypeStruct((8, COLS), f32),
            jax.ShapeDtypeStruct((8, COLS), f32),
            jax.ShapeDtypeStruct((COLS, WIDE), bf16),
        ),
        in_specs=[vmem] * 3,
        out_specs=(hbm,) * 8,
        scratch_shapes=[dma((3,))],
        compiler_params=pltpu.CompilerParams(vmem_limit_bytes=4 * 1024 * 1024),
        name="write",
    )(*passed)
    return (*outs[:3], outs[3].reshape(WIDE, COLS), *outs[4:])


def solution(mesh):
    torus = Mesh(mesh.devices.reshape(4, 4, 2, 4), ("z", "y", "c", "x"))
    split = P(FS, "x")
    whole = P(FS, None)
    return jax.shard_map(
        shards,
        mesh=torus,
        in_specs=(
            split, split, P("x"), P("x"), whole, whole, split, whole, whole,
            split, P("x", FS), split, split, split, split,
        ),
        out_specs=(
            split, split, split, P(None, "x"), P("x", FS), split, split, P("x", None),
        ),
        check_vma=False,
    )
```

```python
import math

import jax
import jax.numpy as jnp
from jax import lax
from jax.experimental import pallas as pl
from jax.experimental.pallas import tpu as pltpu
from jax.sharding import Mesh
from jax.sharding import PartitionSpec as P

MESH = pl.DeviceIdType.MESH
RANK = 256
HV = 2048
FS = ("z", "y", "c")

norm_epsilon = 1e-06
first_decay = 0.9
second_decay = 0.95
learn_rate = 0.1

ROWS = 768
WIDE = 4096
COLS = 512
HEADS_HERE = 4
CHIPS = 16
LANES = 128

f32 = jnp.float32
bf16 = jnp.bfloat16

LEVELS = (
    ((0, 0),),
    ((3, 0), (1, 0), (0, 3), (0, 1)),
    ((2, 0), (3, 3), (3, 1), (1, 3), (1, 1), (0, 2)),
    ((2, 3), (2, 1), (3, 2), (1, 2)),
    ((2, 2),),
)
GROUPS = (
    (),
    (((3, 0),), ((1, 0),), ((0, 3), (0, 1))),
    (((2, 0),), ((3, 3), (3, 1), (1, 3), (1, 1), (0, 2))),
    (((2, 3), (2, 1)), ((3, 2), (1, 2))),
    (((2, 2),),),
)
GROUP_OF = {p: k for k, group in enumerate(sum(GROUPS, ())) for p in group}


def step_kernel(
    first_map, second_map, lambda_head, head_gain, cot_output, layer_input, cot_values,
    factor_value, factor_output, weight_value, weight_output,
    first_value, second_value, first_output, second_output,
    new_weights, moved, copies,
    maps, lam, gain, wide, rights, right_in, factors, other_rows, weights, moments,
    acc, turned, summed, cross_in, squares, cross_sq, last_sq, low_all, ratios, added, back, back_moved,
    load_sem, out_sem, in_sem, send_sem, recv_sem, moment_sem, pass_sem, cross_sem, sq_sem, low_sem,
):
    z, y, c, x = (lax.axis_index(a) for a in ("z", "y", "c", "x"))
    own = 4 * z + y
    mine = 2 * own + c
    partner = (z, y, 1 - c, x)

    def near(z_by, y_by, c_by, x_by):
        return (
            lax.rem(z + z_by, 4), lax.rem(y + y_by, 4), lax.rem(c + c_by, 2), lax.rem(x + x_by, 4)
        )

    def at(dz, dy):
        return 4 * lax.rem(z + dz, 4) + lax.rem(y + dy, 4)

    def place(da, db):
        return at(da * c + db * (1 - c), da * (1 - c) + db * c)

    def chip_at(da, db):
        return near(da * c + db * (1 - c), da * (1 - c) + db * c, 0, 0)

    def remote(source, target, sent, arrived, device):
        return pltpu.make_async_remote_copy(
            source, target, sent, arrived, device_id=device, device_id_type=MESH
        )

    def arrive(block, semaphore):
        remote(block, block, out_sem.at[0], semaphore, partner).wait_recv()

    def sent_off(block, semaphore):
        remote(block, block, semaphore, in_sem.at[0], partner).wait_send()

    def load(k, source, target):
        copy = pltpu.make_async_copy(source, target, load_sem.at[k])
        copy.start()

    def loaded(k, target):
        pltpu.make_async_copy(target, target, load_sem.at[k]).wait()

    value_args = (first_value, second_value, layer_input)
    output_args = (first_output, second_output, cot_output)

    def columns(ref, j):
        return ref.at[:, pl.ds(LANES * j, LANES)]

    def rows(ref, j):
        return ref.at[pl.ds(LANES * j, LANES)]

    def load_first(own_factor, other_factor):
        load(0, own_factor, factors.at[mine])
        load(8, other_factor, other_rows)

    def load_later(args, weight, pieces):
        load(1, args[2], wide.at[0])
        load(2, args[0], moments.at[mine, 0])
        load(2, args[1], moments.at[mine, 1])
        for j in range(4):
            load(3, pieces(weight, j), rows(weights.at[c], j))

    pl.when(c == 0)(lambda: load_first(factor_value, factor_output))
    pl.when(c == 1)(lambda: load_first(factor_output, factor_value))
    barrier = pltpu.get_barrier_semaphore()
    greeted = [chip_at(1, 0), chip_at(3, 0), chip_at(0, 1), chip_at(0, 3), partner]
    greeted += [near(0, 0, 0, dx) for dx in (1, 2, 3)]
    for device in greeted:
        pl.semaphore_signal(barrier, inc=1, device_id=device, device_id_type=MESH)
    load(4, first_map, maps.at[0])
    load(4, second_map, maps.at[1])
    load(5, lambda_head, lam)
    load(6, head_gain, gain)
    pl.when(c == 0)(lambda: load_later(value_args, weight_value, columns))
    pl.when(c == 1)(lambda: load_later(output_args, weight_output, rows))
    load(7, cot_values, rights.at[0])
    pl.semaphore_wait(barrier, len(greeted))

    def hand(k, source, target):
        remote(source, target, out_sem.at[k], in_sem.at[k], partner).start()

    def hand_later(args, weight, pieces):
        hand(1, args[2], wide.at[1])
        hand(2, args[0], moments.at[mine, 0])
        hand(2, args[1], moments.at[mine, 1])
        for j in range(4):
            hand(3, pieces(weight, j), rows(weights.at[c], j))

    loaded(8, other_rows)
    hand(0, other_rows, factors.at[mine])

    class Gather:
        def __init__(self, stage, arrived, blocks, parts, passed=None):
            self.blocks, self.passed, self.sent = blocks, passed, send_sem.at[stage]
            self.parts, self.size = parts, blocks.shape[1] // parts
            self.pieces = [(g, s) for g in (0, 1) for s in range(parts)]
            self.counts = [0, 0]
            self.arrived = arrived

        def piece(self, g, s, da, db):
            block = self.blocks.at[2 * place(da, db) + (c if g == 0 else 1 - c)]
            return block.at[pl.ds(self.size * s, self.size)]

        def fire(self, g, s, da, db, *ways):
            block = self.piece(g, s, da, db)
            for way in ways:
                ra, rb = da, db
                by = 1 if way[1] == "+" else 3
                if way[0] == "a":
                    device, ra = chip_at(by, 0), (da - by) % 4
                else:
                    device, rb = chip_at(0, by), (db - by) % 4
                arrived = self.arrived.at[self.parts * g + s, GROUP_OF[ra, rb]]
                remote(block, block, self.sent.at[g], arrived, device).start()
                self.counts[g] += 1
            if self.passed is not None:
                remote(block, block, self.sent.at[g], self.passed, partner).start()
                self.counts[g] += 1

        def start(self, g, s):
            self.fire(g, s, 0, 0, "b+", "b-", "a+", "a-")

        def take(self, g, s, group):
            whole = self.blocks.at[pl.ds(0, len(group)), pl.ds(0, self.size)]
            arrive(whole, self.arrived.at[self.parts * g + s, GROUP_OF[group[0]]])
            even = (g + s) % 2 == 0
            for da, db in group:
                ways = []
                if db == 0:
                    if da == (3 if even else 1):
                        ways.append("a+" if even else "a-")
                    ways += ["b+", "b-"]
                elif db == (3 if (da in (0, 1)) == even else 1):
                    ways.append("b+" if db == 3 else "b-")
                self.fire(g, s, da, db, *ways)

        def take_level(self, level, only=None):
            for g, s in self.pieces:
                if only in (None, g):
                    for group in GROUPS[level]:
                        self.take(g, s, group)

        def finish(self):
            for g in (0, 1):
                sent_off(self.blocks.at[pl.ds(0, self.counts[g] // self.parts)], self.sent.at[g])

    loaded(0, factors.at[mine])
    gather = Gather(0, recv_sem, factors, 2)
    gather.start(0, 0)
    gather.start(0, 1)
    pl.when(c == 0)(lambda: hand_later(output_args, weight_output, rows))
    pl.when(c == 1)(lambda: hand_later(value_args, weight_value, columns))
    loaded(4, maps)
    loaded(5, lam)
    loaded(6, gain)
    width = COLS // HEADS_HERE
    for h in range(HEADS_HERE):
        span = pl.ds(h * width, width)
        differ = maps[0, :, span].astype(f32) - lam[h] * maps[1, :, span].astype(f32)
        mean = jnp.sum(differ * differ, axis=-1, keepdims=True) * (1.0 / width)
        scaled = differ * lax.rsqrt(mean + norm_epsilon)
        rights[1, :, span] = (scaled * gain[span][None, :]).astype(bf16)
    arrive(factors.at[mine], in_sem.at[0])
    gather.start(1, 0)
    gather.start(1, 1)
    loaded(7, rights.at[0])
    hand(4, rights.at[1 - c], right_in)

    def project(t, *chips, fresh=False):
        left = [wide[t, :, pl.ds(pl.multiple_of(p * 256, 256), 256)] for p in chips]
        right = [factors[pl.ds(2 * p, 2)].reshape(256, RANK) for p in chips]
        if len(chips) > 1:
            left, right = [jnp.concatenate(left, axis=1)], [jnp.concatenate(right, axis=0)]
        part = jnp.dot(left[0], right[0], preferred_element_type=f32)
        acc[t] = part if fresh else acc[t] + part

    PAIRS = (
        None,
        (((1, 0), (3, 0)), ((0, 1), (0, 3))),
        (((2, 0), (0, 2)), ((1, 1), (3, 3)), ((1, 3), (3, 1))),
        (((2, 1), (2, 3)), ((1, 2), (3, 2))),
    )

    def project_pairs(t, level, *which):
        for k in which:
            (z0, y0), (z1, y1) = PAIRS[level][k]
            project(t, at(z0, y0), at(z1, y1))

    gather.take_level(1)
    loaded(1, wide.at[0])
    project(0, own, fresh=True)
    gather.take_level(2, 0)
    project_pairs(0, 1, 0)
    gather.take_level(2, 1)
    project_pairs(0, 1, 1)
    gather.take_level(3, 0)
    arrive(wide.at[1], in_sem.at[1])
    project(1, own, fresh=True)
    project_pairs(1, 1, 0, 1)
    gather.take_level(3, 1)
    loaded(2, moments.at[mine])
    arrive(moments.at[mine], in_sem.at[2])
    moment_gather = Gather(1, moment_sem, moments, 1)
    moment_gather.start(0, 0)
    moment_gather.start(1, 0)
    project_pairs(0, 2, 0, 1, 2)
    project_pairs(1, 2, 0, 1, 2)
    for t in (0, 1):
        project_pairs(t, 3, 0, 1)
    gather.take_level(4)
    for t in (0, 1):
        project(t, at(2, 2))

    arrive(right_in, in_sem.at[4])
    product = None
    for t in (0, 1):
        flat = acc[t].T
        high = flat.astype(bf16)
        turned[t, :RANK] = high
        turned[t, RANK:] = (flat - high.astype(f32)).astype(bf16)
        right = rights[c] if t == 0 else right_in[...]
        part = jnp.dot(turned[t], right, preferred_element_type=f32)
        product = part if t == 0 else product + part
    summed[...] = (product[:RANK] + product[RANK:]).reshape(CHIPS, 16, COLS)

    offsets = sorted(
        ((dz, dy) for dz in range(4) for dy in range(4) if (dz, dy) != (0, 0)),
        key=lambda o: -(min(o[0], 4 - o[0]) + min(o[1], 4 - o[1])),
    )
    for k, (dz, dy) in enumerate(offsets):
        remote(
            summed.at[at(dz, dy)], cross_in.at[k], cross_sem.at[0], cross_sem.at[1],
            near(dz, dy, 0, 0),
        ).start()
    moment_gather.take_level(1)
    arrive(cross_in, cross_sem.at[1])
    total = summed[own]
    for k in range(len(offsets)):
        total = total + cross_in[k]
    low_all[own] = total

    def fold(value):
        value = value[:8] + value[8:]
        return sum(value[:, LANES * j : LANES * (j + 1)] for j in range(COLS // LANES))

    squares[0, :1] = jnp.sum(fold(total * total), axis=0, keepdims=True)
    everyone = [(dz, dy, dc) for dz, dy in offsets for dc in (1, 0)] + [(0, 0, 1)]
    for k, (dz, dy, dc) in enumerate(everyone):
        remote(
            squares.at[0, pl.ds(0, 1)], cross_sq.at[pl.ds(k, 1)], sq_sem.at[0, 0], sq_sem.at[0, 1], near(dz, dy, dc, 0)
        ).start()
    def send_low(block, way):
        for by in (2, 1, 3):
            device = chip_at(by, 0) if way == 0 else chip_at(0, by)
            remote(block, block, low_sem.at[way, 0], low_sem.at[way, 1], device).start()

    send_low(low_all.at[own], 0)
    send_low(low_all.at[own], 1)
    moment_gather.take_level(2)
    arrive(low_all.at[pl.ds(0, 3)], low_sem.at[0, 1])
    for k in (2, 1, 3):
        send_low(low_all.at[place(k, 0)], 1)
    arrive(cross_sq.at[pl.ds(0, 31)], sq_sem.at[0, 1])
    cross_sq[31:] = squares[0, :1]
    squares[1, :1] = jnp.sum(cross_sq[...], axis=0, keepdims=True)
    for k, dx in enumerate((2, 1, 3)):
        remote(
            squares.at[1, pl.ds(0, 1)], last_sq.at[pl.ds(k, 1)], sq_sem.at[1, 0], sq_sem.at[1, 1], near(0, 0, 0, dx)
        ).start()
    moment_gather.take_level(3)
    arrive(weights.at[0], in_sem.at[3])
    loaded(3, weights.at[0])
    arrive(low_all.at[pl.ds(0, 12)], low_sem.at[1, 1])
    arrive(last_sq.at[pl.ds(0, 3)], sq_sem.at[1, 1])
    whole = squares[1, :1] + last_sq[0:1] + last_sq[1:2] + last_sq[2:3]
    square_sum = jnp.sum(whole, axis=1, keepdims=True)
    clip = jnp.minimum(1.0, math.sqrt(RANK * HV) * lax.rsqrt(square_sum + norm_epsilon))

    moment_gather.take_level(4)
    def moved_by(low, first_old, second_old):
        scaled = clip * low
        first_new = first_decay * first_old + (1.0 - first_decay) * scaled
        second_new = second_decay * second_old + (1.0 - second_decay) * scaled * scaled
        return first_new, second_new

    step = 2
    for k in range(0, CHIPS, step):
        low = low_all[k : k + step].reshape(16 * step, COLS)
        first_old = moments[2 * k : 2 * (k + step), 0].reshape(16 * step, COLS)
        second_old = moments[2 * k : 2 * (k + step), 1].reshape(16 * step, COLS)
        first_new, second_new = moved_by(low, first_old, second_old)
        ratio = first_new * lax.rsqrt(second_new)
        high = ratio.astype(bf16)
        ratios[0, 16 * k : 16 * (k + step)] = high
        ratios[1, 16 * k : 16 * (k + step)] = (ratio - high.astype(f32)).astype(bf16)
    left = factors[pl.ds(2 * own, 2)].reshape(256, RANK)
    added[...] = (
        jnp.dot(left, ratios[0], preferred_element_type=f32)
        + jnp.dot(left, ratios[1], preferred_element_type=f32)
    ).reshape(2, LANES, COLS)

    spread = Gather(2, recv_sem, copies.at[c], 2, passed=pass_sem.at[0])
    for g in (0, 1):
        core = c if g == 0 else 1 - c
        for j in range(4):
            span = pl.ds(LANES * j, LANES)
            update = added[core, :, span]
            update = jnp.where(c == 0, update, update.T)
            fresh = weights[core, span] - learn_rate * update
            copies[c, 2 * own + core, span] = fresh.astype(bf16)
            if g == 0:
                new_weights[c, span] = fresh
            else:
                back[span] = fresh
            if j % 2 == 1:
                spread.start(g, j // 2)
    for g in (0, 1):
        core = c if g == 0 else 1 - c
        first_new, second_new = moved_by(
            low_all[own, pl.ds(8 * core, 8)], moments[2 * own + core, 0], moments[2 * own + core, 1]
        )
        target = moved.at[c] if g == 0 else back_moved
        target[0] = first_new
        target[1] = second_new
    hand(5, back, new_weights.at[c])
    hand(6, back_moved, moved.at[c])
    gather.finish()
    moment_gather.finish()
    sent_off(factors.at[0], out_sem.at[0])
    sent_off(wide.at[0], out_sem.at[1])
    sent_off(moments.at[0], out_sem.at[2])
    sent_off(weights.at[0], out_sem.at[3])
    sent_off(right_in, out_sem.at[4])
    sent_off(cross_in, cross_sem.at[0])
    sent_off(cross_sq.at[pl.ds(0, 31)], sq_sem.at[0, 0])
    sent_off(last_sq.at[pl.ds(0, 3)], sq_sem.at[1, 0])
    sent_off(low_all.at[pl.ds(0, 3)], low_sem.at[0, 0])
    sent_off(low_all.at[pl.ds(0, 12)], low_sem.at[1, 0])
    for level in (1, 2, 3, 4):
        spread.take_level(level)
    sent_off(back, out_sem.at[5])
    sent_off(back_moved, out_sem.at[6])
    arrive(back, in_sem.at[5])
    arrive(back_moved, in_sem.at[6])
    arrive(copies.at[0], pass_sem.at[0])
    spread.finish()


def write_kernel(new_weights, moved, copies, *rest):
    outs, sem = rest[:8], rest[8]
    new_v, first_v, second_v, copy_v, new_o, first_o, second_o, copy_o = outs
    for j in range(4):
        span = pl.ds(LANES * j, LANES)
        pltpu.make_async_copy(copies.at[0, :, span], copy_v.at[:, :, span], sem.at[0]).start()
        pltpu.make_async_copy(new_weights.at[0, span], new_v.at[:, span], sem.at[1]).start()
    for k in range(2 * CHIPS):
        target = copy_o.at[:, pl.ds(LANES * k, LANES)]
        pltpu.make_async_copy(copies.at[1, k], target, sem.at[0]).start()
    pltpu.make_async_copy(new_weights.at[1], new_o, sem.at[1]).start()
    for k, target in enumerate((first_v, second_v, first_o, second_o)):
        pltpu.make_async_copy(moved.at[k // 2, k % 2], target, sem.at[2]).start()
    for k, source in enumerate((copies, new_weights, moved)):
        pltpu.make_async_copy(source, source, sem.at[k]).wait()


def shards(*args):
    hbm = pl.BlockSpec(memory_space=pltpu.HBM)
    vmem = pl.BlockSpec(memory_space=pltpu.VMEM)
    dma = pltpu.SemaphoreType.DMA
    passed = pl.pallas_call(
        step_kernel,
        out_shape=(
            pltpu.VMEM((2, COLS, LANES), f32),
            pltpu.VMEM((2, 2, 8, COLS), f32),
            pltpu.VMEM((2, 2 * CHIPS, COLS, LANES), bf16),
        ),
        in_specs=[hbm] * 15,
        out_specs=(vmem,) * 3,
        scratch_shapes=[
            pltpu.VMEM((2, ROWS, COLS), bf16),
            pltpu.SMEM((HEADS_HERE,), f32),
            pltpu.VMEM((COLS,), f32),
            pltpu.VMEM((2, ROWS, WIDE), bf16),
            pltpu.VMEM((2, ROWS, COLS), bf16),
            pltpu.VMEM((ROWS, COLS), bf16),
            pltpu.VMEM((2 * CHIPS, LANES, RANK), bf16),
            pltpu.VMEM((LANES, RANK), bf16),
            pltpu.VMEM((2, COLS, LANES), f32),
            pltpu.VMEM((2 * CHIPS, 2, 8, COLS), f32),
            pltpu.VMEM((2, ROWS, RANK), f32),
            pltpu.VMEM((2, 2 * RANK, ROWS), bf16),
            pltpu.VMEM((CHIPS, 16, COLS), f32),
            pltpu.VMEM((CHIPS - 1, 16, COLS), f32),
            pltpu.VMEM((2, 8, LANES), f32),
            pltpu.VMEM((2 * CHIPS, LANES), f32),
            pltpu.VMEM((8, LANES), f32),
            pltpu.VMEM((CHIPS, 16, COLS), f32),
            pltpu.VMEM((2, RANK, COLS), bf16),
            pltpu.VMEM((2, LANES, COLS), f32),
            pltpu.VMEM((COLS, LANES), f32),
            pltpu.VMEM((2, 8, COLS), f32),
            dma((9,)),
            dma((7,)),
            dma((7,)),
            dma((3, 2)),
            dma((4, 8)),
            dma((2, 8)),
            dma((1,)),
            dma((2,)),
            dma((2, 2)),
            dma((2, 2)),
        ],
        compiler_params=pltpu.CompilerParams(
            collective_id=0, has_side_effects=True, vmem_limit_bytes=46 * 1024 * 1024
        ),
        name="step",
    )(*args)
    outs = pl.pallas_call(
        write_kernel,
        out_shape=(
            jax.ShapeDtypeStruct((LANES, COLS), f32),
            jax.ShapeDtypeStruct((8, COLS), f32),
            jax.ShapeDtypeStruct((8, COLS), f32),
            jax.ShapeDtypeStruct((2 * CHIPS, LANES, COLS), bf16),
            jax.ShapeDtypeStruct((COLS, LANES), f32),
            jax.ShapeDtypeStruct((8, COLS), f32),
            jax.ShapeDtypeStruct((8, COLS), f32),
            jax.ShapeDtypeStruct((COLS, WIDE), bf16),
        ),
        in_specs=[vmem] * 3,
        out_specs=(hbm,) * 8,
        scratch_shapes=[dma((3,))],
        compiler_params=pltpu.CompilerParams(vmem_limit_bytes=4 * 1024 * 1024),
        name="write",
    )(*passed)
    return (*outs[:3], outs[3].reshape(WIDE, COLS), *outs[4:])


def solution(mesh):
    torus = Mesh(mesh.devices.reshape(4, 4, 2, 4), ("z", "y", "c", "x"))
    split = P(FS, "x")
    whole = P(FS, None)
    return jax.shard_map(
        shards,
        mesh=torus,
        in_specs=(
            split, split, P("x"), P("x"), whole, whole, split, whole, whole,
            split, P("x", FS), split, split, split, split,
        ),
        out_specs=(
            split, split, split, P(None, "x"), P("x", FS), split, split, P("x", None),
        ),
        check_vma=False,
    )
```

```python
import math

import jax
import jax.numpy as jnp
from jax import lax
from jax.experimental import pallas as pl
from jax.experimental.pallas import tpu as pltpu
from jax.sharding import Mesh
from jax.sharding import PartitionSpec as P

MESH = pl.DeviceIdType.MESH
RANK = 256
HV = 2048
FS = ("z", "y", "c")

norm_epsilon = 1e-06
first_decay = 0.9
second_decay = 0.95
learn_rate = 0.1

ROWS = 768
WIDE = 4096
COLS = 512
HEADS_HERE = 4
CHIPS = 16
LANES = 128

f32 = jnp.float32
bf16 = jnp.bfloat16

LEVELS = (
    ((0, 0),),
    ((3, 0), (1, 0), (0, 3), (0, 1)),
    ((2, 0), (3, 3), (3, 1), (1, 3), (1, 1), (0, 2)),
    ((2, 3), (2, 1), (3, 2), (1, 2)),
    ((2, 2),),
)
GROUPS = (
    (),
    (((3, 0),), ((1, 0),), ((0, 3), (0, 1))),
    (((2, 0),), ((3, 3), (3, 1), (1, 3), (1, 1), (0, 2))),
    (((2, 3), (2, 1)), ((3, 2), (1, 2))),
    (((2, 2),),),
)
GROUP_OF = {p: k for k, group in enumerate(sum(GROUPS, ())) for p in group}


def step_kernel(
    first_map, second_map, lambda_head, head_gain, cot_output, layer_input, cot_values,
    factor_value, factor_output, weight_value, weight_output,
    first_value, second_value, first_output, second_output,
    new_weights, moved, copies,
    maps, lam, gain, wide, rights, right_in, factors, other_rows, weights, moments,
    acc, turned, summed, cross_in, squares, cross_sq, last_sq, low_all, ratios, added, back, back_moved,
    load_sem, out_sem, in_sem, send_sem, recv_sem, moment_sem, pass_sem, cross_sem, sq_sem, low_sem,
):
    z, y, c, x = (lax.axis_index(a) for a in ("z", "y", "c", "x"))
    own = 4 * z + y
    mine = 2 * own + c
    partner = (z, y, 1 - c, x)

    def near(z_by, y_by, c_by, x_by):
        return (
            lax.rem(z + z_by, 4), lax.rem(y + y_by, 4), lax.rem(c + c_by, 2), lax.rem(x + x_by, 4)
        )

    def at(dz, dy):
        return 4 * lax.rem(z + dz, 4) + lax.rem(y + dy, 4)

    def place(da, db):
        return at(da * c + db * (1 - c), da * (1 - c) + db * c)

    def chip_at(da, db):
        return near(da * c + db * (1 - c), da * (1 - c) + db * c, 0, 0)

    def remote(source, target, sent, arrived, device):
        return pltpu.make_async_remote_copy(
            source, target, sent, arrived, device_id=device, device_id_type=MESH
        )

    def arrive(block, semaphore):
        remote(block, block, out_sem.at[0], semaphore, partner).wait_recv()

    def sent_off(block, semaphore):
        remote(block, block, semaphore, in_sem.at[0], partner).wait_send()

    def load(k, source, target):
        copy = pltpu.make_async_copy(source, target, load_sem.at[k])
        copy.start()

    def loaded(k, target):
        pltpu.make_async_copy(target, target, load_sem.at[k]).wait()

    value_args = (first_value, second_value, layer_input)
    output_args = (first_output, second_output, cot_output)

    def columns(ref, j):
        return ref.at[:, pl.ds(LANES * j, LANES)]

    def rows(ref, j):
        return ref.at[pl.ds(LANES * j, LANES)]

    def load_first(own_factor, other_factor):
        load(0, own_factor, factors.at[mine])
        load(8, other_factor, other_rows)

    def load_later(args, weight, pieces):
        load(1, args[2], wide.at[0])
        load(2, args[0], moments.at[mine, 0])
        load(2, args[1], moments.at[mine, 1])
        for j in range(4):
            load(3, pieces(weight, j), rows(weights.at[c], j))

    pl.when(c == 0)(lambda: load_first(factor_value, factor_output))
    pl.when(c == 1)(lambda: load_first(factor_output, factor_value))
    barrier = pltpu.get_barrier_semaphore()
    greeted = [chip_at(1, 0), chip_at(3, 0), chip_at(0, 1), chip_at(0, 3), partner]
    greeted += [near(0, 0, dc, dx) for dx in (1, 2, 3) for dc in (0, 1)]
    for device in greeted:
        pl.semaphore_signal(barrier, inc=1, device_id=device, device_id_type=MESH)
    load(4, first_map, maps.at[0])
    load(4, second_map, maps.at[1])
    load(5, lambda_head, lam)
    load(6, head_gain, gain)
    pl.when(c == 0)(lambda: load_later(value_args, weight_value, columns))
    pl.when(c == 1)(lambda: load_later(output_args, weight_output, rows))
    load(7, cot_values, rights.at[0])
    pl.semaphore_wait(barrier, len(greeted))

    def hand(k, source, target):
        remote(source, target, out_sem.at[k], in_sem.at[k], partner).start()

    def hand_later(args, weight, pieces):
        hand(1, args[2], wide.at[1])
        hand(2, args[0], moments.at[mine, 0])
        hand(2, args[1], moments.at[mine, 1])
        for j in range(4):
            hand(3, pieces(weight, j), rows(weights.at[c], j))

    loaded(8, other_rows)
    hand(0, other_rows, factors.at[mine])

    class Gather:
        def __init__(self, stage, arrived, blocks, parts, passed=None):
            self.blocks, self.passed, self.sent = blocks, passed, send_sem.at[stage]
            self.parts, self.size = parts, blocks.shape[1] // parts
            self.pieces = [(g, s) for g in (0, 1) for s in range(parts)]
            self.counts = [0, 0]
            self.arrived = arrived

        def piece(self, g, s, da, db):
            block = self.blocks.at[2 * place(da, db) + (c if g == 0 else 1 - c)]
            return block.at[pl.ds(self.size * s, self.size)]

        def fire(self, g, s, da, db, *ways):
            block = self.piece(g, s, da, db)
            for way in ways:
                ra, rb = da, db
                by = 1 if way[1] == "+" else 3
                if way[0] == "a":
                    device, ra = chip_at(by, 0), (da - by) % 4
                else:
                    device, rb = chip_at(0, by), (db - by) % 4
                arrived = self.arrived.at[self.parts * g + s, GROUP_OF[ra, rb]]
                remote(block, block, self.sent.at[g], arrived, device).start()
                self.counts[g] += 1
            if self.passed is not None:
                remote(block, block, self.sent.at[g], self.passed, partner).start()
                self.counts[g] += 1

        def start(self, g):
            for s in range(self.parts):
                self.fire(g, s, 0, 0, "b+", "b-", "a+", "a-")

        def take(self, g, s, group):
            whole = self.blocks.at[pl.ds(0, len(group)), pl.ds(0, self.size)]
            arrive(whole, self.arrived.at[self.parts * g + s, GROUP_OF[group[0]]])
            even = (g + s) % 2 == 0
            for da, db in group:
                ways = []
                if db == 0:
                    if da == (3 if even else 1):
                        ways.append("a+" if even else "a-")
                    ways += ["b+", "b-"]
                elif db == (3 if (da in (0, 1)) == even else 1):
                    ways.append("b+" if db == 3 else "b-")
                self.fire(g, s, da, db, *ways)

        def take_level(self, level, only=None):
            for g, s in self.pieces:
                if only in (None, g):
                    for group in GROUPS[level]:
                        self.take(g, s, group)

        def finish(self):
            for g in (0, 1):
                sent_off(self.blocks.at[pl.ds(0, self.counts[g] // self.parts)], self.sent.at[g])

    loaded(0, factors.at[mine])
    gather = Gather(0, recv_sem, factors, 2)
    gather.start(0)
    pl.when(c == 0)(lambda: hand_later(output_args, weight_output, rows))
    pl.when(c == 1)(lambda: hand_later(value_args, weight_value, columns))
    loaded(4, maps)
    loaded(5, lam)
    loaded(6, gain)
    width = COLS // HEADS_HERE
    for h in range(HEADS_HERE):
        span = pl.ds(h * width, width)
        differ = maps[0, :, span].astype(f32) - lam[h] * maps[1, :, span].astype(f32)
        mean = jnp.sum(differ * differ, axis=-1, keepdims=True) * (1.0 / width)
        scaled = differ * lax.rsqrt(mean + norm_epsilon)
        rights[1, :, span] = (scaled * gain[span][None, :]).astype(bf16)
    arrive(factors.at[mine], in_sem.at[0])
    gather.start(1)
    loaded(7, rights.at[0])
    hand(4, rights.at[1 - c], right_in)

    def project(t, *chips, fresh=False):
        left = [wide[t, :, pl.ds(pl.multiple_of(p * 256, 256), 256)] for p in chips]
        right = [factors[pl.ds(2 * p, 2)].reshape(256, RANK) for p in chips]
        if len(chips) > 1:
            left, right = [jnp.concatenate(left, axis=1)], [jnp.concatenate(right, axis=0)]
        part = jnp.dot(left[0], right[0], preferred_element_type=f32)
        acc[t] = part if fresh else acc[t] + part

    PAIRS = (
        None,
        (((1, 0), (3, 0)), ((0, 1), (0, 3))),
        (((2, 0), (0, 2)), ((1, 1), (3, 3)), ((1, 3), (3, 1))),
        (((2, 1), (2, 3)), ((1, 2), (3, 2))),
    )

    def project_pairs(t, level, *which):
        for k in which:
            (z0, y0), (z1, y1) = PAIRS[level][k]
            project(t, at(z0, y0), at(z1, y1))

    gather.take_level(1)
    loaded(1, wide.at[0])
    project(0, own, fresh=True)
    gather.take_level(2, 0)
    project_pairs(0, 1, 0)
    gather.take_level(2, 1)
    project_pairs(0, 1, 1)
    gather.take_level(3, 0)
    arrive(wide.at[1], in_sem.at[1])
    project(1, own, fresh=True)
    project_pairs(1, 1, 0, 1)
    gather.take_level(3, 1)
    loaded(2, moments.at[mine])
    arrive(moments.at[mine], in_sem.at[2])
    moment_gather = Gather(1, moment_sem, moments, 1)
    moment_gather.start(0)
    moment_gather.start(1)
    project_pairs(0, 2, 0, 1, 2)
    project_pairs(1, 2, 0, 1, 2)
    for t in (0, 1):
        project_pairs(t, 3, 0, 1)
    arrive(right_in, in_sem.at[4])
    gather.take_level(4)
    product = None
    for t in (0, 1):
        project(t, at(2, 2))
        flat = acc[t].T
        high = flat.astype(bf16)
        turned[t, :RANK] = high
        turned[t, RANK:] = (flat - high.astype(f32)).astype(bf16)
        right = rights[c] if t == 0 else right_in[...]
        part = jnp.dot(turned[t], right, preferred_element_type=f32)
        product = part if t == 0 else product + part
    summed[...] = (product[:RANK] + product[RANK:]).reshape(CHIPS, 16, COLS)

    offsets = sorted(
        ((dz, dy) for dz in range(4) for dy in range(4) if (dz, dy) != (0, 0)),
        key=lambda o: -(min(o[0], 4 - o[0]) + min(o[1], 4 - o[1])),
    )
    for k, (dz, dy) in enumerate(offsets):
        remote(
            summed.at[at(dz, dy)], cross_in.at[k], cross_sem.at[0], cross_sem.at[1],
            near(dz, dy, 0, 0),
        ).start()
    moment_gather.take_level(1)
    arrive(cross_in, cross_sem.at[1])
    total = summed[own]
    for k in range(len(offsets)):
        total = total + cross_in[k]
    low_all[own] = total

    def fold(value):
        value = value[:8] + value[8:]
        return sum(value[:, LANES * j : LANES * (j + 1)] for j in range(COLS // LANES))

    squares[0] = fold(total * total)
    for k, (dz, dy) in enumerate(offsets):
        remote(
            squares.at[0], cross_sq.at[k], sq_sem.at[0, 0], sq_sem.at[0, 1], near(dz, dy, 0, 0)
        ).start()
    def send_low(block, way):
        for by in (2, 1, 3):
            device = chip_at(by, 0) if way == 0 else chip_at(0, by)
            remote(block, block, low_sem.at[way, 0], low_sem.at[way, 1], device).start()

    send_low(low_all.at[own], 0)
    send_low(low_all.at[own], 1)
    moment_gather.take_level(2)
    arrive(cross_sq, sq_sem.at[0, 1])
    plane = squares[0]
    for k in range(len(offsets)):
        plane = plane + cross_sq[k]
    squares[1] = plane
    for k, (dx, dc) in enumerate(((2, 1), (1, 1), (3, 1), (2, 0), (1, 0), (3, 0), (0, 1))):
        remote(
            squares.at[1], last_sq.at[k], sq_sem.at[1, 0], sq_sem.at[1, 1], near(0, 0, dc, dx)
        ).start()
    arrive(low_all.at[pl.ds(0, 3)], low_sem.at[0, 1])
    for k in (2, 1, 3):
        send_low(low_all.at[place(k, 0)], 1)
    moment_gather.take_level(3)
    arrive(weights.at[0], in_sem.at[3])
    loaded(3, weights.at[0])
    arrive(low_all.at[pl.ds(0, 12)], low_sem.at[1, 1])
    arrive(last_sq, sq_sem.at[1, 1])
    whole = squares[1]
    for k in range(7):
        whole = whole + last_sq[k]
    square_sum = jnp.sum(jnp.sum(whole, axis=1, keepdims=True), axis=0, keepdims=True)
    clip = jnp.minimum(1.0, math.sqrt(RANK * HV) * lax.rsqrt(square_sum + norm_epsilon))

    moment_gather.take_level(4)
    def moved_by(low, first_old, second_old):
        scaled = clip * low
        first_new = first_decay * first_old + (1.0 - first_decay) * scaled
        second_new = second_decay * second_old + (1.0 - second_decay) * scaled * scaled
        return first_new, second_new

    step = 2
    for k in range(0, CHIPS, step):
        low = low_all[k : k + step].reshape(16 * step, COLS)
        first_old = moments[2 * k : 2 * (k + step), 0].reshape(16 * step, COLS)
        second_old = moments[2 * k : 2 * (k + step), 1].reshape(16 * step, COLS)
        first_new, second_new = moved_by(low, first_old, second_old)
        ratio = first_new * lax.rsqrt(second_new)
        high = ratio.astype(bf16)
        ratios[0, 16 * k : 16 * (k + step)] = high
        ratios[1, 16 * k : 16 * (k + step)] = (ratio - high.astype(f32)).astype(bf16)
    left = factors[pl.ds(2 * own, 2)].reshape(256, RANK)
    added[...] = (
        jnp.dot(left, ratios[0], preferred_element_type=f32)
        + jnp.dot(left, ratios[1], preferred_element_type=f32)
    ).reshape(2, LANES, COLS)

    spread = Gather(2, recv_sem, copies.at[c], 2, passed=pass_sem.at[0])
    for g in (0, 1):
        core = c if g == 0 else 1 - c
        for j in range(4):
            span = pl.ds(LANES * j, LANES)
            update = added[core, :, span]
            update = jnp.where(c == 0, update, update.T)
            fresh = weights[core, span] - learn_rate * update
            copies[c, 2 * own + core, span] = fresh.astype(bf16)
            if g == 0:
                new_weights[c, span] = fresh
            else:
                back[span] = fresh
        spread.start(g)
    for g in (0, 1):
        core = c if g == 0 else 1 - c
        first_new, second_new = moved_by(
            low_all[own, pl.ds(8 * core, 8)], moments[2 * own + core, 0], moments[2 * own + core, 1]
        )
        target = moved.at[c] if g == 0 else back_moved
        target[0] = first_new
        target[1] = second_new
    hand(5, back, new_weights.at[c])
    hand(6, back_moved, moved.at[c])
    gather.finish()
    moment_gather.finish()
    sent_off(factors.at[0], out_sem.at[0])
    sent_off(wide.at[0], out_sem.at[1])
    sent_off(moments.at[0], out_sem.at[2])
    sent_off(weights.at[0], out_sem.at[3])
    sent_off(right_in, out_sem.at[4])
    sent_off(cross_in, cross_sem.at[0])
    sent_off(cross_sq, sq_sem.at[0, 0])
    sent_off(last_sq, sq_sem.at[1, 0])
    sent_off(low_all.at[pl.ds(0, 3)], low_sem.at[0, 0])
    sent_off(low_all.at[pl.ds(0, 12)], low_sem.at[1, 0])
    for level in (1, 2, 3, 4):
        spread.take_level(level)
    sent_off(back, out_sem.at[5])
    sent_off(back_moved, out_sem.at[6])
    arrive(back, in_sem.at[5])
    arrive(back_moved, in_sem.at[6])
    arrive(copies.at[0], pass_sem.at[0])
    spread.finish()


def write_kernel(new_weights, moved, copies, *rest):
    outs, sem = rest[:8], rest[8]
    new_v, first_v, second_v, copy_v, new_o, first_o, second_o, copy_o = outs
    for j in range(4):
        span = pl.ds(LANES * j, LANES)
        pltpu.make_async_copy(copies.at[0, :, span], copy_v.at[:, :, span], sem.at[0]).start()
        pltpu.make_async_copy(new_weights.at[0, span], new_v.at[:, span], sem.at[1]).start()
    for k in range(2 * CHIPS):
        target = copy_o.at[:, pl.ds(LANES * k, LANES)]
        pltpu.make_async_copy(copies.at[1, k], target, sem.at[0]).start()
    pltpu.make_async_copy(new_weights.at[1], new_o, sem.at[1]).start()
    for k, target in enumerate((first_v, second_v, first_o, second_o)):
        pltpu.make_async_copy(moved.at[k // 2, k % 2], target, sem.at[2]).start()
    for k, source in enumerate((copies, new_weights, moved)):
        pltpu.make_async_copy(source, source, sem.at[k]).wait()


def shards(*args):
    hbm = pl.BlockSpec(memory_space=pltpu.HBM)
    vmem = pl.BlockSpec(memory_space=pltpu.VMEM)
    dma = pltpu.SemaphoreType.DMA
    passed = pl.pallas_call(
        step_kernel,
        out_shape=(
            pltpu.VMEM((2, COLS, LANES), f32),
            pltpu.VMEM((2, 2, 8, COLS), f32),
            pltpu.VMEM((2, 2 * CHIPS, COLS, LANES), bf16),
        ),
        in_specs=[hbm] * 15,
        out_specs=(vmem,) * 3,
        scratch_shapes=[
            pltpu.VMEM((2, ROWS, COLS), bf16),
            pltpu.SMEM((HEADS_HERE,), f32),
            pltpu.VMEM((COLS,), f32),
            pltpu.VMEM((2, ROWS, WIDE), bf16),
            pltpu.VMEM((2, ROWS, COLS), bf16),
            pltpu.VMEM((ROWS, COLS), bf16),
            pltpu.VMEM((2 * CHIPS, LANES, RANK), bf16),
            pltpu.VMEM((LANES, RANK), bf16),
            pltpu.VMEM((2, COLS, LANES), f32),
            pltpu.VMEM((2 * CHIPS, 2, 8, COLS), f32),
            pltpu.VMEM((2, ROWS, RANK), f32),
            pltpu.VMEM((2, 2 * RANK, ROWS), bf16),
            pltpu.VMEM((CHIPS, 16, COLS), f32),
            pltpu.VMEM((CHIPS - 1, 16, COLS), f32),
            pltpu.VMEM((2, 8, LANES), f32),
            pltpu.VMEM((CHIPS - 1, 8, LANES), f32),
            pltpu.VMEM((7, 8, LANES), f32),
            pltpu.VMEM((CHIPS, 16, COLS), f32),
            pltpu.VMEM((2, RANK, COLS), bf16),
            pltpu.VMEM((2, LANES, COLS), f32),
            pltpu.VMEM((COLS, LANES), f32),
            pltpu.VMEM((2, 8, COLS), f32),
            dma((9,)),
            dma((7,)),
            dma((7,)),
            dma((3, 2)),
            dma((4, 8)),
            dma((2, 8)),
            dma((1,)),
            dma((2,)),
            dma((2, 2)),
            dma((2, 2)),
        ],
        compiler_params=pltpu.CompilerParams(
            collective_id=0, has_side_effects=True, vmem_limit_bytes=46 * 1024 * 1024
        ),
        name="step",
    )(*args)
    outs = pl.pallas_call(
        write_kernel,
        out_shape=(
            jax.ShapeDtypeStruct((LANES, COLS), f32),
            jax.ShapeDtypeStruct((8, COLS), f32),
            jax.ShapeDtypeStruct((8, COLS), f32),
            jax.ShapeDtypeStruct((2 * CHIPS, LANES, COLS), bf16),
            jax.ShapeDtypeStruct((COLS, LANES), f32),
            jax.ShapeDtypeStruct((8, COLS), f32),
            jax.ShapeDtypeStruct((8, COLS), f32),
            jax.ShapeDtypeStruct((COLS, WIDE), bf16),
        ),
        in_specs=[vmem] * 3,
        out_specs=(hbm,) * 8,
        scratch_shapes=[dma((3,))],
        compiler_params=pltpu.CompilerParams(vmem_limit_bytes=4 * 1024 * 1024),
        name="write",
    )(*passed)
    return (*outs[:3], outs[3].reshape(WIDE, COLS), *outs[4:])


def solution(mesh):
    torus = Mesh(mesh.devices.reshape(4, 4, 2, 4), ("z", "y", "c", "x"))
    split = P(FS, "x")
    whole = P(FS, None)
    return jax.shard_map(
        shards,
        mesh=torus,
        in_specs=(
            split, split, P("x"), P("x"), whole, whole, split, whole, whole,
            split, P("x", FS), split, split, split, split,
        ),
        out_specs=(
            split, split, split, P(None, "x"), P("x", FS), split, split, P("x", None),
        ),
        check_vma=False,
    )
```
